512 devices in a mesh: kv: 64 (over z, y), tp: 8 (over x, core).
Axes of the slice: x: 4, y: 4, z: 16, core: 2. Of those that a mesh axis runs over, the one named last changes fastest.
Arguments:
- tokens: bfloat16 [24, 4096], P(None, 'kv'), may hold values from -60 to 60
- gain_first: bfloat16 [4096], P('kv'), may hold values from 0.099609375 to 1.8984375
- gate_first: bfloat16 [4096, 11264], P('kv', 'tp'), may hold values from -0.09375 to 0.09375
- up_first: bfloat16 [4096, 11264], P('kv', 'tp'), may hold values from -0.09375 to 0.09375
- down_first: bfloat16 [11264, 4096], P('tp', 'kv'), may hold values from -0.0546875 to 0.0546875
- gain_mixer: bfloat16 [4096], P('kv'), may hold values from 0.099609375 to 1.8984375
- query_weight: bfloat16 [4096, 2048], P('kv', 'tp'), may hold values from -0.09375 to 0.09375
- key_weight: bfloat16 [4096, 2048], P('kv', 'tp'), may hold values from -0.25 to 0.25
- value_weight: bfloat16 [4096, 2048], P('kv', 'tp'), may hold values from -0.09375 to 0.09375
- forget_weight: bfloat16 [4096, 16], replicated, may hold values from -0.09375 to 0.09375
- forget_bias: float32 [16], replicated, may hold values from -1 to 2
- key_cache: bfloat16 [24, 8192, 16, 128], P(None, 'kv', 'tp'), may hold values from -2000 to 2000
- value_cache: bfloat16 [24, 8192, 16, 128], P(None, 'kv', 'tp'), may hold values from -6 to 6
- forget_sum: float32 [24, 16, 8192], P(None, 'tp', 'kv'), may hold values from -1024 to 0, as said below
- out_weight: bfloat16 [2048, 4096], P('tp', 'kv'), may hold values from -0.5 to 0.5
- gain_second: bfloat16 [4096], P('kv'), may hold values from 0.099609375 to 1.8984375
- gate_second: bfloat16 [4096, 11264], P('kv', 'tp'), may hold values from -0.09375 to 0.09375
- up_second: bfloat16 [4096, 11264], P('kv', 'tp'), may hold values from -0.09375 to 0.09375
- down_second: bfloat16 [11264, 4096], P('tp', 'kv'), may hold values from -0.0546875 to 0.0546875
Outputs:
- updated: bfloat16 [24, 4096], P(None, 'kv')
The draws below stay inside these ranges and needn't reach their ends.
Inputs may be any that keep to these rules, and one draw needn't show every extreme that they name: forget_sum[b, h, s] is the sum of the log forget gates of the cached positions after s, up to the last cached one, for sequence b and head h; it never falls with s, is at most 0, and rises to 0 at the last cached position.
All inputs are finite; a program needn't handle non-finite values.
Results may differ from the reference program's by a relative error of at most 0.02.
Values may be sent and summed in bfloat16 or wider, within the bound.
A program may use at most 64 MiB of HBM per device.

```python
import math
import jax
import jax.numpy as jnp
from jax import lax

D = 4096
HEAD_TOTAL = 16
HEAD_DIM = 128
FF = 11264
BLOCK = 128
SEQUENCE_TOTAL = 24
CACHE_LENGTH = 8192
N_KV = 64
N_TP = 8


def draw_tokens(key, part):
    random_subkeys = jax.random.split(jax.random.fold_in(key, 11), 4)
    row_scale = jnp.exp(jax.random.uniform(random_subkeys[0], (SEQUENCE_TOTAL, 1), jnp.float32, math.log(0.3), math.log(3.0)))
    column_ramp = jnp.exp(jnp.linspace(0.0, math.log(3.0), D, dtype=jnp.float32))[None, :]
    roughness = jax.random.uniform(random_subkeys[1], (1, D), jnp.float32, 0.5, 1.5)
    values = jax.random.normal(random_subkeys[3], (SEQUENCE_TOTAL, D), jnp.float32) * row_scale * column_ramp * roughness
    return jnp.clip(values, -60.0, 60.0).astype(jnp.bfloat16)


def draw_key_cache(key, part):
    random_subkeys = jax.random.split(jax.random.fold_in(key, 17), 6)
    cache_shape = (SEQUENCE_TOTAL, CACHE_LENGTH, HEAD_TOTAL, HEAD_DIM)
    base_keys = jax.random.normal(random_subkeys[0], cache_shape, jnp.float32)
    chosen = jax.random.uniform(random_subkeys[1], (SEQUENCE_TOTAL, 1, HEAD_TOTAL, 1), jnp.float32) < 0.5
    strength = jnp.exp(jax.random.uniform(random_subkeys[2], (SEQUENCE_TOTAL, 1, HEAD_TOTAL, 1), jnp.float32, math.log(40.0), math.log(300.0)))
    first_spot = jax.random.randint(random_subkeys[3], (SEQUENCE_TOTAL, 1, HEAD_TOTAL, 1), 0, CACHE_LENGTH - 1)
    cache_position = jnp.arange(CACHE_LENGTH, dtype=jnp.int32).reshape(1, CACHE_LENGTH, 1, 1)
    direction = jax.random.normal(random_subkeys[4], (SEQUENCE_TOTAL, 1, HEAD_TOTAL, HEAD_DIM), jnp.float32)
    nudge_dir = jax.random.normal(random_subkeys[5], (SEQUENCE_TOTAL, 1, HEAD_TOTAL, HEAD_DIM), jnp.float32)
    planted = jnp.where(cache_position == first_spot, strength * direction, base_keys)
    planted = jnp.where(cache_position == first_spot + 1, strength * direction + 1.5 * nudge_dir, planted)
    base_keys = jnp.where(chosen, planted, base_keys)
    return jnp.clip(base_keys, -2000.0, 2000.0).astype(jnp.bfloat16)


def draw_forget_sum(key, part):
    random_subkeys = jax.random.split(jax.random.fold_in(key, 23), 7)
    slow_share = 0.5
    slow_flag = jax.random.uniform(random_subkeys[0], (SEQUENCE_TOTAL, HEAD_TOTAL, 1), jnp.float32) < slow_share
    slow_total = jnp.exp(jax.random.uniform(random_subkeys[1], (SEQUENCE_TOTAL, HEAD_TOTAL, 1), jnp.float32, math.log(0.7), math.log(2.5)))
    fast_rate = jnp.exp(jax.random.uniform(random_subkeys[2], (SEQUENCE_TOTAL, HEAD_TOTAL, 1), jnp.float32, math.log(0.01), math.log(1.0 / 30.0)))
    decay_rate = jnp.where(slow_flag, slow_total / CACHE_LENGTH, fast_rate)
    device_factor = jnp.exp(jax.random.uniform(random_subkeys[3], (SEQUENCE_TOTAL, HEAD_TOTAL, N_KV), jnp.float32, math.log(0.5), math.log(2.0)))
    device_factor = jnp.repeat(device_factor, CACHE_LENGTH // N_KV, axis=2)
    roughness = jax.random.uniform(random_subkeys[4], (SEQUENCE_TOTAL, HEAD_TOTAL, CACHE_LENGTH), jnp.float32, 0.5, 1.5)
    descent_steps = -decay_rate * device_factor * roughness
    spike_location = jax.random.randint(random_subkeys[5], (SEQUENCE_TOTAL, HEAD_TOTAL, 3), 0, CACHE_LENGTH)
    spike_depth = jnp.log(jax.random.uniform(random_subkeys[6], (SEQUENCE_TOTAL, HEAD_TOTAL, 3), jnp.float32, 0.5, 0.8))
    cache_position = jnp.arange(CACHE_LENGTH, dtype=jnp.int32)
    spike_list = jnp.sum(jnp.where(cache_position[None, None, None, :] == spike_location[..., None], spike_depth[..., None], 0.0), axis=2)
    descent_steps = descent_steps + jnp.where(slow_flag, spike_list, 0.0)
    running = jnp.cumsum(descent_steps, axis=2)
    return running[:, :, -1:] - running


def block_scale(own_key, dims, cuts, low, top_value):
    factor_of = 1.0
    for axis_at, parts in cuts:
        heights = jax.random.uniform(jax.random.fold_in(jax.random.fold_in(own_key, 6), axis_at), (parts,), jnp.float32, low / len(cuts), top_value / len(cuts))
        factor_of = factor_of * jnp.repeat(jnp.exp(heights), dims[axis_at] // parts).reshape((-1,) + (1,) * (len(dims) - 1 - axis_at))
    return factor_of


def scatter_about(rng, extent, deviation, most, cuts=(), kind=jnp.bfloat16):
    gain = block_scale(rng, extent, cuts, -0.22, 0.18) if cuts else 1.0
    result = jax.random.normal(rng, extent, jnp.float32) * deviation * gain
    return jnp.minimum(jnp.maximum(result, -most), most).astype(kind)


def setup_inputs(seed: int = 0) -> dict:
    keys = jax.random.split(jax.random.key(seed), 20)
    tokens = draw_tokens(jax.random.fold_in(keys[19], 71), 0)
    gain_first = jnp.clip(1.0 + 0.18 * jax.random.normal(keys[1], (D,), jnp.float32), 0.099609375, 1.8984375).astype(jnp.bfloat16)
    gate_first = scatter_about(keys[2], (D, FF), D ** -0.5, 0.09375, ((0, 64), (1, 8)))
    up_first = scatter_about(keys[3], (D, FF), D ** -0.5, 0.09375, ((0, 64), (1, 8)))
    down_first = scatter_about(keys[4], (FF, D), FF ** -0.5, 0.0546875, ((0, 8), (1, 64)))
    gain_mixer = jnp.clip(1.0 + 0.18 * jax.random.normal(keys[5], (D,), jnp.float32), 0.099609375, 1.8984375).astype(jnp.bfloat16)
    query_weight = scatter_about(keys[6], (D, HEAD_TOTAL * HEAD_DIM), D ** -0.5, 0.09375, ((0, 64), (1, 8)))
    key_weight = scatter_about(keys[7], (D, HEAD_TOTAL * HEAD_DIM), (D // 8) ** -0.5, 0.25, ((0, 64), (1, 8)))
    value_weight = scatter_about(keys[8], (D, HEAD_TOTAL * HEAD_DIM), D ** -0.5, 0.09375, ((0, 64), (1, 8)))
    forget_weight = scatter_about(keys[9], (D, HEAD_TOTAL), D ** -0.5, 0.09375)
    forget_bias = jnp.clip(jax.random.uniform(keys[10], (HEAD_TOTAL,), jnp.float32, -1.0, 2.0), -1.0, 2.0)
    key_cache = draw_key_cache(jax.random.fold_in(keys[19], 71), 0)
    value_cache = scatter_about(keys[12], (SEQUENCE_TOTAL, CACHE_LENGTH, HEAD_TOTAL, HEAD_DIM), 1.0, 6.0, ((1, 64), (2, 8)))
    forget_sum = draw_forget_sum(jax.random.fold_in(keys[19], 71), 0)
    out_weight = scatter_about(keys[14], (HEAD_TOTAL * HEAD_DIM, D), (HEAD_TOTAL * HEAD_DIM // 16) ** -0.5, 0.5, ((0, 8), (1, 64)))
    gain_second = jnp.clip(1.0 + 0.18 * jax.random.normal(keys[15], (D,), jnp.float32), 0.099609375, 1.8984375).astype(jnp.bfloat16)
    gate_second = scatter_about(keys[16], (D, FF), D ** -0.5, 0.09375, ((0, 64), (1, 8)))
    up_second = scatter_about(keys[17], (D, FF), D ** -0.5, 0.09375, ((0, 64), (1, 8)))
    down_second = scatter_about(keys[18], (FF, D), FF ** -0.5, 0.0546875, ((0, 8), (1, 64)))
    return dict(tokens=tokens, gain_first=gain_first, gate_first=gate_first, up_first=up_first, down_first=down_first, gain_mixer=gain_mixer, query_weight=query_weight, key_weight=key_weight, value_weight=value_weight, forget_weight=forget_weight, forget_bias=forget_bias, key_cache=key_cache, value_cache=value_cache, forget_sum=forget_sum, out_weight=out_weight, gain_second=gain_second, gate_second=gate_second, up_second=up_second, down_second=down_second)


EPSILON = 1e-06

def row_factor(tokens):
    widened = tokens.astype(jnp.float32)
    return lax.rsqrt(lax.optimization_barrier(jnp.mean(widened * widened, axis=1, keepdims=True)) + EPSILON)

def scaled_rows(tokens, norm_gain):
    return (tokens.astype(jnp.float32) * norm_gain.astype(jnp.float32)).astype(jnp.bfloat16)

def grouped_sum(left, right, groups):
    seq_count = left.shape[0]
    left_groups = left.reshape(seq_count, groups, -1).astype(jnp.float32)
    right_groups = right.reshape(groups, -1, right.shape[1]).astype(jnp.float32)
    partial_value = jnp.einsum('bgf,gfd->gbd', left_groups, right_groups).astype(jnp.bfloat16)
    partial_value = lax.optimization_barrier(partial_value)
    return lax.optimization_barrier(jnp.sum(partial_value.astype(jnp.float32), axis=0))

def feed_forward(tokens, norm_gain, gate_matrix, up_matrix, down_matrix):
    factor = row_factor(tokens)
    scaled = scaled_rows(tokens, norm_gain)
    gate_value = factor * jnp.dot(scaled, gate_matrix, preferred_element_type=jnp.float32)
    up_value = factor * jnp.dot(scaled, up_matrix, preferred_element_type=jnp.float32)
    hidden = (jax.nn.silu(gate_value) * up_value).astype(jnp.bfloat16)
    summed = grouped_sum(hidden, down_matrix, N_TP)
    return (tokens.astype(jnp.float32) + 0.5 * summed).astype(jnp.bfloat16)

def attend_one(items):
    query_rows, new_key, new_value, log_gate, cached_keys, cached_values, forget_row = items
    inverse = query_rows.shape[1] ** (-0.5)
    scores = jnp.einsum('hd,lhd->hl', query_rows.astype(jnp.float32), cached_keys.astype(jnp.float32)) * inverse
    scores = scores + forget_row + log_gate[:, None]
    head_count = scores.shape[0]
    blocks = scores.shape[1] // BLOCK
    scores = scores.reshape(head_count, blocks, BLOCK)
    highest = lax.optimization_barrier(jnp.max(scores, axis=2))
    weights = jnp.exp(scores - highest[..., None]).astype(jnp.bfloat16)
    block_sum = lax.optimization_barrier(jnp.sum(weights.astype(jnp.float32), axis=2))
    block_value = jnp.einsum('hcs,cshd->hcd', weights.astype(jnp.float32), cached_values.reshape(blocks, BLOCK, head_count, -1).astype(jnp.float32))
    own_score = lax.optimization_barrier(jnp.sum(query_rows.astype(jnp.float32) * new_key.astype(jnp.float32), axis=1)) * inverse
    ceiling = jnp.maximum(lax.optimization_barrier(jnp.max(highest, axis=1)), own_score)
    cache_scale = jnp.exp(highest - ceiling[:, None])
    own_scale = jnp.exp(own_score - ceiling)
    numerator = lax.optimization_barrier(jnp.sum(cache_scale[..., None] * block_value, axis=1)) + own_scale[:, None] * new_value.astype(jnp.float32)
    denominator = lax.optimization_barrier(jnp.sum(cache_scale * block_sum, axis=1)) + own_scale
    return (numerator / denominator[:, None]).astype(jnp.bfloat16)

def mix_tokens(tokens, norm_gain, query_weight, key_weight, value_weight, forget_weight, forget_bias, key_cache, value_cache, forget_sum, out_weight):
    factor = row_factor(tokens)
    scaled = scaled_rows(tokens, norm_gain)
    seq_count = tokens.shape[0]
    head_count = key_cache.shape[2]

    def project(matrix):
        product = factor * jnp.dot(scaled, matrix, preferred_element_type=jnp.float32)
        return product.astype(jnp.bfloat16).reshape(seq_count, head_count, -1)
    query_rows = project(query_weight)
    new_key = project(key_weight)
    new_value = project(value_weight)
    log_gate = jax.nn.log_sigmoid(factor * jnp.dot(scaled, forget_weight, preferred_element_type=jnp.float32) + forget_bias)
    attended = lax.map(attend_one, (query_rows, new_key, new_value, log_gate, key_cache, value_cache, forget_sum))
    summed = grouped_sum(attended.reshape(seq_count, -1), out_weight, N_TP)
    return (tokens.astype(jnp.float32) + summed).astype(jnp.bfloat16)

def reference(tokens, gain_first, gate_first, up_first, down_first, gain_mixer, query_weight, key_weight, value_weight, forget_weight, forget_bias, key_cache, value_cache, forget_sum, out_weight, gain_second, gate_second, up_second, down_second):
    first_out = feed_forward(tokens, gain_first, gate_first, up_first, down_first)
    mixed = mix_tokens(first_out, gain_mixer, query_weight, key_weight, value_weight, forget_weight, forget_bias, key_cache, value_cache, forget_sum, out_weight)
    return feed_forward(mixed, gain_second, gate_second, up_second, down_second)
```

```python
import functools

import jax
import jax.numpy as jnp
from jax import lax
from jax.experimental import pallas as pl
from jax.experimental.pallas import tpu as pltpu
from jax.sharding import PartitionSpec as P

MESH = pl.DeviceIdType.MESH
EPSILON = 1e-06
SIDE = 4
GROUP = 6
TILE = 8
ROWS = SIDE * TILE
LANES = 128
F32 = jnp.float32
BF16 = jnp.bfloat16


def dot(left, right):
    return lax.dot_general(left, right, (((1,), (0,)), ((), ())), preferred_element_type=F32)


def dot_rows(left, right):
    return lax.dot_general(left, right, (((1,), (1,)), ((), ())), preferred_element_type=F32)


def iota(shape, dim):
    return lax.broadcasted_iota(jnp.int32, shape, dim)


def far_first(count):
    return sorted(range(1, count), key=lambda k: (-min(k, count - k), k))


def split_value(value, pieces):
    parts = []
    for _ in range(pieces):
        part = value.astype(BF16)
        parts.append(part)
        value = value - part.astype(F32)
    return parts


def layer_kernel(
    ranks,
    features,
    bias,
    tokens_hbm,
    gain_a_hbm,
    gate_a_hbm,
    up_a_hbm,
    down_a_hbm,
    gain_m_hbm,
    wq_hbm,
    wk_hbm,
    wv_hbm,
    forget_hbm,
    keys_hbm,
    values_hbm,
    decay_hbm,
    wo_hbm,
    gain_b_hbm,
    gate_b_hbm,
    up_b_hbm,
    down_b_hbm,
    out_ref,
    tokens,
    gain_a,
    gate_a,
    up_a,
    down_a,
    gain_m,
    wq,
    wk,
    wv,
    forget,
    keys,
    values,
    decay,
    wo,
    gain_b,
    gate_b,
    up_b,
    down_b,
    load_sem,
    bufs_a,
    bufs_b,
    bufs_m,
):
    kv_count, tp_count = ranks
    depth = kv_count // SIDE
    kv, tp = lax.axis_index("kv"), lax.axis_index("tp")
    z, y = lax.div(kv, SIDE), lax.rem(kv, SIDE)
    chunks = gate_a.shape[1] // LANES

    def at_z(k):
        return lax.rem(z + k, depth)

    def at_y(k):
        return lax.rem(y + k, SIDE)

    def at_tp(k):
        return lax.rem(tp + k, tp_count)

    z_steps, y_steps, tp_steps = far_first(depth), far_first(SIDE), far_first(tp_count)

    barrier = pltpu.get_barrier_semaphore()
    for k in z_steps:
        pl.semaphore_signal(barrier, inc=1, device_id=(at_z(k) * SIDE + y, tp), device_id_type=MESH)
    for k in y_steps:
        pl.semaphore_signal(barrier, inc=1, device_id=(z * SIDE + at_y(k), tp), device_id_type=MESH)
    for k in tp_steps:
        pl.semaphore_signal(barrier, inc=1, device_id=(kv, at_tp(k)), device_id_type=MESH)

    block = pl.multiple_of(lax.div(kv, 2) * LANES, LANES)
    pairs = [
        (tokens_hbm, tokens),
        (gain_a_hbm, gain_a),
        (gate_a_hbm, gate_a),
        (up_a_hbm, up_a),
        (down_a_hbm, down_a),
        (decay_hbm, decay),
        (gain_m_hbm, gain_m),
        (wq_hbm, wq),
        (wk_hbm, wk),
        (wv_hbm, wv),
        (forget_hbm.at[:, pl.ds(block, LANES)], forget),
        (keys_hbm, keys),
        (values_hbm, values),
        (wo_hbm, wo),
        (gain_b_hbm, gain_b),
        (gate_b_hbm, gate_b),
        (up_b_hbm, up_b),
        (down_b_hbm, down_b),
    ]
    loads = [pltpu.make_async_copy(a, b, load_sem.at[n]) for n, (a, b) in enumerate(pairs)]
    for load in loads:
        load.start()
    waiting = list(loads)

    def loaded(count):
        for _ in range(count):
            waiting.pop(0).wait()

    sent = []

    def push(source, target, send_sem, recv_sem, device):
        copy = pltpu.make_async_remote_copy(
            src_ref=source,
            dst_ref=target,
            send_sem=send_sem,
            recv_sem=recv_sem,
            device_id=device,
            device_id_type=MESH,
        )
        copy.start()
        return copy

    def along_y(source_of, target, sems):
        send_sem, recv_sem = sems
        for k in y_steps:
            far = at_y(k)
            sent.append((None, push(
                source_of(far), target.at[y], send_sem.at[k], recv_sem.at[y], (z * SIDE + far, tp)
            )))

    def from_y(target, sems):
        for k in y_steps:
            far = at_y(k)
            slot = target.at[far]
            pltpu.make_async_copy(slot, slot, sems[1].at[far]).wait()

    def along_z(target, sems):
        send_sem, recv_sem = sems
        for k in z_steps:
            far = at_z(k)
            sent.append((None, push(
                target.at[z], target.at[z], send_sem.at[k], recv_sem.at[z], (far * SIDE + y, tp)
            )))

    def from_z(target, sems):
        for k in reversed(z_steps):
            far = at_z(k)
            slot = target.at[far]
            pltpu.make_async_copy(slot, slot, sems[1].at[far]).wait()

    def total_over_tp(partial, target, sems):
        send_sem, recv_sem = sems
        target[tp] = partial.astype(BF16)
        for k in tp_steps:
            sent.append((None, push(
                target.at[tp], target.at[tp], send_sem.at[k], recv_sem.at[tp], (kv, at_tp(k))
            )))
        for k in reversed(tp_steps):
            slot = target.at[at_tp(k)]
            pltpu.make_async_copy(slot, slot, recv_sem.at[at_tp(k)]).wait()
        total = target[0].astype(F32)
        for k in range(1, tp_count):
            total = total + target[k].astype(F32)
        return total

    sub, lane = iota((TILE, LANES), 0), iota((TILE, LANES), 1)

    def column(line, first):
        picked = jnp.where(lane == first + y * TILE + sub, jnp.broadcast_to(line, (TILE, LANES)), 0.0)
        return jnp.sum(picked, axis=1, keepdims=True)

    def squares_of(x):
        return split_value(x * x, 2)

    def owner(j):
        return lax.div(j * depth, chunks)

    def chunk_of(place):
        return lax.div(chunks * place + depth - 1, depth)

    def owns(place):
        j = chunk_of(place)
        return jnp.logical_and(j < chunks, owner(j) == place)

    def feed_forward(x, gain, gate, up, down, bufs):
        sy, ry, sz, rz, hy, rt, y_sems, zs_sems, zg_sems, h_sems, t_sems = bufs
        scaled = (x * gain[...].astype(F32)).astype(BF16)
        ones = jnp.ones((TILE, x.shape[1]), BF16)
        blank = jnp.zeros((LANES - ROWS, x.shape[1]), BF16)
        high, low = squares_of(x)
        squares = dot_rows(ones, jnp.concatenate([high, blank])) + dot_rows(
            ones, jnp.concatenate([low, blank])
        )
        for u, weight in enumerate((gate, up)):
            product = dot(scaled, weight[...])
            for g in range(SIDE):
                for j in range(chunks):
                    tile = product[g * TILE : (g + 1) * TILE, j * LANES : (j + 1) * LANES]
                    if u == 0:
                        tile = jnp.where(sub == GROUP, squares, tile)
                    sy[g, j, u] = tile.astype(BF16)
        if bufs is bufs_a:
            pl.semaphore_wait(barrier, len(z_steps) + len(y_steps) + len(tp_steps))
        along_y(lambda far: sy.at[far], ry, y_sems)
        from_y(ry, y_sems)
        total = sy[y].astype(F32)
        for k in y_steps:
            total = total + ry[at_y(k)].astype(F32)
        sz[...] = total.astype(BF16)
        for k in z_steps:
            far = at_z(k)

            @pl.when(owns(far))
            def _():
                push(
                    sz.at[chunk_of(far)],
                    rz.at[z],
                    zs_sems[0].at[k],
                    zs_sems[1].at[z],
                    (far * SIDE + y, tp),
                )

            sent.append((owns(far), (sz.at[0], zs_sems[0].at[k])))

        @pl.when(owns(z))
        def _():
            mine = chunk_of(z)
            from_z(rz, zs_sems)
            rz[z] = sz[mine]
            both = rz[0].astype(F32)
            for k in range(1, depth):
                both = both + rz[k].astype(F32)
            gate_sum, up_sum = both[0], both[1]
            factor = column(lax.rsqrt(gate_sum[GROUP : GROUP + 1] / features + EPSILON), 0)
            gate_value, up_value = factor * gate_sum, factor * up_sum
            hidden = gate_value / (1.0 + jnp.exp(-gate_value)) * up_value
            hy[y, mine] = jnp.where(sub < GROUP, hidden, 0.0).astype(BF16)
            for k in z_steps:
                push(
                    hy.at[y, mine],
                    hy.at[y, mine],
                    zg_sems[0].at[k],
                    zg_sems[1].at[mine],
                    (at_z(k) * SIDE + y, tp),
                )

        for k in z_steps:
            sent.append((owns(z), (hy.at[y, 0], zg_sems[0].at[k])))
        for k in reversed(z_steps):
            far = at_z(k)

            @pl.when(owns(far))
            def _():
                slot = hy.at[y, chunk_of(far)]
                pltpu.make_async_copy(slot, slot, zg_sems[1].at[chunk_of(far)]).wait()

        along_y(lambda far: hy.at[y], hy, h_sems)
        from_y(hy, h_sems)
        hidden = jnp.concatenate(
            [hy[:, j].astype(F32).reshape(ROWS, LANES).astype(BF16) for j in range(chunks)], axis=1
        )
        summed = total_over_tp(dot_rows(hidden, down[...]), rt, t_sems)
        return (x + 0.5 * summed).astype(BF16).astype(F32)

    def mix(x):
        (
            sq, rq, zq, zkv, qf, sa, ra, rst, za, zst, af, rt,
            q_sems, zq_sems, zkv_sems, qf_sems, a_sems, st_sems, za_sems, zst_sems, af_sems, t_sems,
        ) = bufs_m
        seqs, positions, width = keys.shape[0], decay.shape[2], x.shape[1]
        inverse = LANES ** (-0.5)

        scaled = (x * gain_m[...].astype(F32)).astype(BF16)
        high, low = squares_of(x)
        blank = jnp.zeros((ROWS, width), BF16)
        half = jnp.where(lax.rem(kv, 2) == 0, forget[:, :width].astype(F32), forget[:, width:].astype(F32))
        heads = forget.shape[0]
        r8, c8 = iota((TILE, heads), 0), iota((TILE, heads), 1)
        pick = jnp.where((r8 >= 1) & (r8 <= 2) & (c8 == 2 * tp + r8 - 1), 1.0, 0.0).astype(BF16)
        lines = dot(pick, half.astype(BF16))
        lines = jnp.where(iota((TILE, width), 0) == 0, 1.0, lines).astype(BF16)
        terms = dot_rows(lines, jnp.concatenate([high, scaled, scaled, blank]))
        extra = dot_rows(lines, jnp.concatenate([low, blank, blank, blank]))
        own_line = jnp.where(sub == lax.shift_right_logical(lane, 5), terms + jnp.where(lane < ROWS, extra, 0.0), 0.0)
        side_line = jnp.sum(own_line, axis=0, keepdims=True)
        for u, weight in enumerate((wq, wk, wv)):
            product = dot(scaled, weight[...])
            for g in range(SIDE):
                for h in range(2):
                    tile = product[g * TILE : (g + 1) * TILE, h * LANES : (h + 1) * LANES]
                    if u == 0 and h == 0:
                        tile = jnp.where(sub == GROUP, jnp.broadcast_to(side_line, (TILE, LANES)), tile)
                    sq[g, 2 * u + h] = tile.astype(BF16)
        along_y(lambda far: sq.at[far], rq, q_sems)
        from_y(rq, q_sems)
        total = sq[y].astype(F32)
        for k in y_steps:
            total = total + rq[at_y(k)].astype(F32)
        total = total.astype(BF16)
        zq[z] = total[:2]
        along_z(zq, zq_sems)
        zkv[z] = total[2:]
        along_z(zkv, zkv_sems)

        from_z(zq, zq_sems)
        both = zq[0].astype(F32)
        for k in range(1, depth):
            both = both + zq[k].astype(F32)
        line = both[0][GROUP : GROUP + 1]
        factor = column(lax.rsqrt(line / features + EPSILON), 0)
        query = [jnp.where(sub < GROUP, factor * both[h], 0.0).astype(BF16) for h in range(2)]
        for h in range(2):
            qf[y, h] = query[h]
        along_y(lambda far: qf.at[y], qf, qf_sems)
        log_gate = []
        for h in range(2):
            gate = factor * column(line, ROWS * (h + 1)) + bias[2 * tp + h]
            log_gate.append(jnp.minimum(gate, 0.0) - jnp.log(1.0 + jnp.exp(-jnp.abs(gate))))

        from_y(qf, qf_sems)
        lane2 = iota((TILE, 2 * positions), 1)
        even = lax.rem(lane2, 2) == 0
        sub2 = iota((TILE, 2 * positions), 0)
        stats = jnp.zeros((1, LANES), F32)
        for g in range(SIDE):
            pair = jnp.concatenate([qf[g, 0].astype(F32), qf[g, 1].astype(F32)]).astype(BF16)
            scores = jnp.zeros((TILE, 2 * positions), F32)
            for i in range(GROUP):
                found = dot_rows(pair, keys[g * GROUP + i])
                found = jnp.where(even, found[:TILE], found[TILE:])
                scores = jnp.where(sub2 == i, found, scores)
            scores = scores * inverse + spread[g * TILE : (g + 1) * TILE]
            tops = [
                jnp.max(jnp.where(even if h == 0 else ~even, scores, -jnp.inf), axis=1, keepdims=True)
                for h in range(2)
            ]
            weights = jnp.exp(scores - jnp.where(even, tops[0], tops[1])).astype(BF16).astype(F32)
            parts = [jnp.where(even, weights, 0.0), jnp.where(even, 0.0, weights)]
            sums = [jnp.sum(part, axis=1, keepdims=True) for part in parts]
            both_parts = jnp.concatenate(parts).astype(BF16)
            mixed = [jnp.zeros((TILE, LANES), F32) for _ in range(2)]
            for i in range(GROUP):
                found = dot(both_parts, values[g * GROUP + i])
                for h in range(2):
                    mixed[h] = jnp.where(sub == i, found[h * TILE : (h + 1) * TILE], mixed[h])
            for h in range(2):
                sa[g, h] = (mixed[h] / sums[h]).astype(BF16)
                level = tops[h] + jnp.log(sums[h])
                stats = stats + jnp.sum(
                    jnp.where(lane == ROWS * h + g * TILE + sub, level, 0.0), axis=0, keepdims=True
                )
        rst[y] = stats
        along_y(lambda far: sa.at[far], ra, a_sems)
        along_y(lambda far: rst.at[y], rst, st_sems)
        from_y(rst, st_sems)
        from_y(ra, a_sems)

        def merged(levels, parts):
            top = functools.reduce(jnp.maximum, levels)
            shares = [jnp.exp(level - top) for level in levels]
            whole = sum(shares[1:], shares[0])
            value = sum((a * b for a, b in zip(shares[1:], parts[1:])), shares[0] * parts[0])
            return value / whole, top + jnp.log(whole)

        spots = [y] + [at_y(k) for k in y_steps]
        stats = jnp.zeros((1, LANES), F32)
        for h in range(2):
            levels = [column(rst[spot], ROWS * h) for spot in spots]
            parts = [sa[y, h].astype(F32)] + [ra[spot, h].astype(F32) for spot in spots[1:]]
            value, level = merged(levels, parts)
            za[z, h] = value.astype(BF16)
            stats = stats + jnp.sum(
                jnp.where(lane == ROWS * h + y * TILE + sub, level, 0.0), axis=0, keepdims=True
            )
        zst[z] = stats
        along_z(zst, zst_sems)
        along_z(za, za_sems)

        from_z(zkv, zkv_sems)
        both = zkv[0].astype(F32)
        for k in range(1, depth):
            both = both + zkv[k].astype(F32)
        fresh = [jnp.where(sub < GROUP, factor * both[u], 0.0).astype(BF16).astype(F32) for u in range(4)]
        own_level = [
            jnp.sum(query[h].astype(F32) * fresh[h], axis=1, keepdims=True) * inverse for h in range(2)
        ]
        from_z(zst, zst_sems)
        from_z(za, za_sems)
        for h in range(2):
            levels = [column(zst[k], ROWS * h) + log_gate[h] for k in range(depth)] + [own_level[h]]
            parts = [za[k, h].astype(F32) for k in range(depth)] + [fresh[2 + h]]
            af[y, h] = merged(levels, parts)[0].astype(BF16)
        along_y(lambda far: af.at[y], af, af_sems)
        from_y(af, af_sems)
        attended = jnp.concatenate(
            [af[:, h].astype(F32).reshape(ROWS, LANES).astype(BF16) for h in range(2)], axis=1
        )
        summed = total_over_tp(dot_rows(attended, wo[...]), rt, t_sems)
        return (x + summed).astype(BF16).astype(F32)

    seqs = tokens.shape[0]
    to_rows = iota((ROWS, seqs), 0)
    seat = lax.shift_right_logical(to_rows, 3) * GROUP + (to_rows & 7)
    place = jnp.where(((to_rows & 7) < GROUP) & (seat == iota((ROWS, seqs), 1)), 1.0, 0.0).astype(BF16)

    loaded(4)
    x = dot(place, tokens[...])
    loaded(1)
    loaded(1)
    positions = decay.shape[2]
    spread = jnp.zeros((ROWS, 2 * positions), F32)
    pieces = [split_value(decay[:, h, :], 3) for h in range(2)]
    for n in range(3):
        woven = jnp.zeros((seqs, 2 * positions), F32)
        for h in range(2):
            weave = jnp.where(
                iota((positions, 2 * positions), 1) == 2 * iota((positions, 2 * positions), 0) + h, 1.0, 0.0
            ).astype(BF16)
            woven = woven + dot(pieces[h][n], weave)
        spread = spread + dot(place, woven.astype(BF16))

    first = feed_forward(x, gain_a, gate_a, up_a, down_a, bufs_a)

    loaded(8)
    second = mix(first)
    loaded(4)
    last = feed_forward(second, gain_b, gate_b, up_b, down_b, bufs_b)

    back = iota((seqs, ROWS), 1)
    seat = lax.shift_right_logical(back, 3) * GROUP + (back & 7)
    lift = jnp.where(((back & 7) < GROUP) & (seat == iota((seqs, ROWS), 0)), 1.0, 0.0).astype(BF16)
    out_ref[...] = dot(lift, last.astype(BF16)).astype(BF16)

    for condition, copy in sent:
        if condition is None:
            copy.wait_send()
        else:
            ref, sem = copy

            @pl.when(condition)
            def _():
                pltpu.make_async_copy(ref, ref, sem).wait()


def on_device(
    ranks,
    tokens,
    gain_first,
    gate_first,
    up_first,
    down_first,
    gain_mixer,
    query_weight,
    key_weight,
    value_weight,
    forget_weight,
    forget_bias,
    key_cache,
    value_cache,
    forget_sum,
    out_weight,
    gain_second,
    gate_second,
    up_second,
    down_second,
):
    kv_count, tp_count = ranks
    depth = kv_count // SIDE
    seqs, length = key_cache.shape[:2]
    chunks = gate_first.shape[1] // LANES
    width = tokens.shape[1]
    dma = pltpu.SemaphoreType.DMA

    def flat(cache):
        return cache.reshape(seqs, 2 * length, LANES)

    operands = [
        tokens,
        gain_first.reshape(1, -1),
        gate_first,
        up_first,
        down_first.T,
        gain_mixer.reshape(1, -1),
        query_weight,
        key_weight,
        value_weight,
        forget_weight.T,
        flat(key_cache),
        flat(value_cache),
        forget_sum,
        out_weight.T,
        gain_second.reshape(1, -1),
        gate_second,
        up_second,
        down_second.T,
    ]
    held = [pltpu.VMEM(a.shape, a.dtype) for a in operands]
    held[9] = pltpu.VMEM((forget_weight.shape[1], LANES), BF16)

    def tiles(*dims):
        return pltpu.VMEM((*dims, TILE, LANES), BF16)

    def pair(count, other=None):
        return (dma((count,)), dma((other or count,)))

    def bufs():
        return (
            tiles(SIDE, chunks, 2),
            tiles(SIDE, chunks, 2),
            tiles(chunks, 2),
            tiles(depth, 2),
            tiles(SIDE, chunks),
            pltpu.VMEM((tp_count, ROWS, width), BF16),
            pair(SIDE),
            pair(depth),
            pair(depth, chunks),
            pair(SIDE),
            pair(tp_count),
        )

    mix_bufs = (
        tiles(SIDE, 6),
        tiles(SIDE, 6),
        tiles(depth, 2),
        tiles(depth, 4),
        tiles(SIDE, 2),
        tiles(SIDE, 2),
        tiles(SIDE, 2),
        pltpu.VMEM((SIDE, 1, LANES), F32),
        tiles(depth, 2),
        pltpu.VMEM((depth, 1, LANES), F32),
        tiles(SIDE, 2),
        pltpu.VMEM((tp_count, ROWS, width), BF16),
        pair(SIDE),
        pair(depth),
        pair(depth),
        pair(SIDE),
        pair(SIDE),
        pair(SIDE),
        pair(depth),
        pair(depth),
        pair(SIDE),
        pair(tp_count),
    )
    return pl.pallas_call(
        functools.partial(layer_kernel, ranks, width * kv_count),
        out_shape=jax.ShapeDtypeStruct(tokens.shape, BF16),
        in_specs=[pl.BlockSpec(memory_space=pltpu.SMEM)]
        + [pl.BlockSpec(memory_space=pltpu.HBM)] * len(operands),
        out_specs=pl.BlockSpec(memory_space=pltpu.VMEM),
        scratch_shapes=held + [dma((len(operands),)), bufs(), bufs(), mix_bufs],
        compiler_params=pltpu.CompilerParams(
            collective_id=0, has_side_effects=True, vmem_limit_bytes=48 * 1024 * 1024
        ),
        name="layer",
    )(forget_bias, *operands)


def solution(mesh):
    ranks = (mesh.shape["kv"], mesh.shape["tp"])
    kv, tp = "kv", "tp"
    in_specs = (
        P(None, kv),
        P(kv),
        P(kv, tp),
        P(kv, tp),
        P(tp, kv),
        P(kv),
        P(kv, tp),
        P(kv, tp),
        P(kv, tp),
        P(),
        P(),
        P(None, kv, tp, None),
        P(None, kv, tp, None),
        P(None, tp, kv),
        P(tp, kv),
        P(kv),
        P(kv, tp),
        P(kv, tp),
        P(tp, kv),
    )
    return jax.shard_map(
        functools.partial(on_device, ranks),
        mesh=mesh,
        in_specs=in_specs,
        out_specs=P(None, kv),
        check_vma=False,
    )
```

```python
import functools

import jax
import jax.numpy as jnp
from jax import lax
from jax.experimental import pallas as pl
from jax.experimental.pallas import tpu as pltpu
from jax.sharding import PartitionSpec as P

MESH = pl.DeviceIdType.MESH
EPSILON = 1e-06
SIDE = 4
GROUP = 6
TILE = 8
ROWS = SIDE * TILE
LANES = 128
F32 = jnp.float32
BF16 = jnp.bfloat16


def dot(left, right):
    return lax.dot_general(left, right, (((1,), (0,)), ((), ())), preferred_element_type=F32)


def dot_rows(left, right):
    return lax.dot_general(left, right, (((1,), (1,)), ((), ())), preferred_element_type=F32)


def iota(shape, dim):
    return lax.broadcasted_iota(jnp.int32, shape, dim)


def far_first(count):
    return sorted(range(1, count), key=lambda k: (-min(k, count - k), k))


def split_value(value, pieces):
    parts = []
    for _ in range(pieces):
        part = value.astype(BF16)
        parts.append(part)
        value = value - part.astype(F32)
    return parts


def layer_kernel(
    ranks,
    features,
    bias,
    tokens_hbm,
    gain_a_hbm,
    gate_a_hbm,
    up_a_hbm,
    down_a_hbm,
    gain_m_hbm,
    wq_hbm,
    wk_hbm,
    wv_hbm,
    forget_hbm,
    keys_hbm,
    values_hbm,
    decay_hbm,
    wo_hbm,
    gain_b_hbm,
    gate_b_hbm,
    up_b_hbm,
    down_b_hbm,
    out_ref,
    tokens,
    gain_a,
    gate_a,
    up_a,
    gain_m,
    gain_b,
    forget,
    keys,
    values,
    decay,
    down_a,
    gates_b,
    down_b,
    w_all,
    wo_all,
    down_a_all,
    gates_b_all,
    down_b_all,
    load_sem,
    tiles_y,
    tiles_all,
    sy,
    ry,
    ff_a,
    ff_b,
    mix_bufs,
    t_one,
    t_two,
    t_three,
    first_all,
    tok_sems,
    y_sems,
    down_a_sems,
    w_sems,
    wo_sems,
    gates_b_sems,
    down_b_sems,
    first_sems,
):
    kv_count, tp_count = ranks
    depth = kv_count // SIDE
    kv, tp = lax.axis_index("kv"), lax.axis_index("tp")
    z, y = lax.div(kv, SIDE), lax.rem(kv, SIDE)
    chunks = gate_a.shape[1] // LANES
    share = down_a.shape[0] // SIDE
    pieces = share * SIDE
    width = tokens.shape[1]
    slab = SIDE * width
    seqs = tokens.shape[0]
    positions = decay.shape[2]

    def at_z(k):
        return lax.rem(z + k, depth)

    def at_y(k):
        return lax.rem(y + k, SIDE)

    def at_tp(k):
        return lax.rem(tp + k, tp_count)

    z_steps, y_steps = far_first(depth), far_first(SIDE)
    plane = sorted(
        [(a, b) for a in range(SIDE) for b in range(tp_count) if a or b],
        key=lambda s: (-min(s[0], SIDE - s[0]) - min(s[1], tp_count - s[1]) / 2, s),
    )

    barrier = pltpu.get_barrier_semaphore()
    for k in z_steps:
        pl.semaphore_signal(barrier, inc=1, device_id=(at_z(k) * SIDE + y, tp), device_id_type=MESH)
    for a, b in plane:
        pl.semaphore_signal(barrier, inc=1, device_id=(z * SIDE + at_y(a), at_tp(b)), device_id_type=MESH)

    def columns(ref, j):
        return ref.at[:, pl.ds(j * LANES, LANES)]

    groups = {
        "tokens": [(tokens_hbm, tokens), (gain_a_hbm, gain_a), (gain_m_hbm, gain_m), (gain_b_hbm, gain_b)],
        "gate_a": [(gate_a_hbm, gate_a)],
        "up_a": [(up_a_hbm, up_a)],
        "down_a": [(columns(down_a_hbm, j), down_a.at[j]) for j in range(chunks)],
        "decay": [(decay_hbm, decay)],
        "w": [(wq_hbm, w_all.at[0, y]), (wk_hbm, w_all.at[1, y]), (wv_hbm, w_all.at[2, y])],
        "wo": [(wo_hbm, wo_all.at[y])],
        "forget": [(forget_hbm.at[:, pl.ds(pl.multiple_of(z * slab, slab), slab)], forget)],
        "keys": [(keys_hbm, keys)],
        "values": [(values_hbm, values)],
        "gates_b": [(columns(gate_b_hbm, j), gates_b.at[j, 0]) for j in range(chunks)]
        + [(columns(up_b_hbm, j), gates_b.at[j, 1]) for j in range(chunks)],
        "down_b": [(columns(down_b_hbm, j), down_b.at[j]) for j in range(chunks)],
    }
    loads, count = {}, 0
    for name, copies in groups.items():
        loads[name] = []
        for a, b in copies:
            load = pltpu.make_async_copy(a, b, load_sem.at[count])
            load.start()
            loads[name].append(load)
            count += 1

    def loaded(*names):
        for name in names:
            for load in loads.pop(name):
                load.wait()

    sent = []

    def push(source, target, send_sem, recv_sem, device):
        copy = pltpu.make_async_remote_copy(
            src_ref=source,
            dst_ref=target,
            send_sem=send_sem,
            recv_sem=recv_sem,
            device_id=device,
            device_id_type=MESH,
        )
        copy.start()
        return copy

    def await_slot(slot, sem):
        pltpu.make_async_copy(slot, slot, sem).wait()

    def along_y(source_of, target_of, sems):
        for k in y_steps:
            far = at_y(k)
            sent.append((None, push(
                source_of(far), target_of(y), sems[0].at[k], sems[1].at[y], (z * SIDE + far, tp)
            )))

    def from_y(target_of, sems):
        for k in y_steps:
            far = at_y(k)
            await_slot(target_of(far), sems[1].at[far])

    def along_z(target, sems):
        for k in z_steps:
            far = at_z(k)
            sent.append((None, push(
                target.at[z], target.at[z], sems[0].at[k], sems[1].at[z], (far * SIDE + y, tp)
            )))

    def from_z(target, sems):
        for k in reversed(z_steps):
            far = at_z(k)
            await_slot(target.at[far], sems[1].at[far])

    def over_plane(source_of, target, sems):
        for n, (a, b) in enumerate(plane):
            far = at_y(a)
            sent.append((None, push(
                source_of(far), target.at[y, tp], sems[0].at[n], sems[1].at[y, tp], (z * SIDE + far, at_tp(b))
            )))

    def from_plane(target, sems):
        for a, b in reversed(plane):
            await_slot(target.at[at_y(a), at_tp(b)], sems[1].at[at_y(a), at_tp(b)])

    sub, lane = iota((TILE, LANES), 0), iota((TILE, LANES), 1)

    def column(line, first):
        picked = jnp.where(lane == first + sub, jnp.broadcast_to(line, (TILE, LANES)), 0.0)
        return jnp.sum(picked, axis=1, keepdims=True)

    def as_line(values, first):
        shape = (values.shape[0], LANES)
        spread_out = jnp.where(iota(shape, 1) == first + iota(shape, 0), values, 0.0)
        return jnp.sum(spread_out, axis=0, keepdims=True)

    def row_sum(x):
        return jnp.sum(x, axis=1, keepdims=True)

    def owner(p):
        return lax.div(p * depth, pieces)

    def piece_of(place):
        return lax.div(pieces * place + depth - 1, depth)

    def owns(place):
        p = piece_of(place)
        return jnp.logical_and(p < pieces, owner(p) == place)

    def send_pieces(bufs, n):
        sz, rz, hz, rs_sems, ag_sems = bufs
        for k in z_steps:
            far = at_z(k)
            p = piece_of(far)

            @pl.when(jnp.logical_and(owns(far), lax.div(p, SIDE) == n))
            def _():
                push(sz.at[p], rz.at[z], rs_sems[0].at[k], rs_sems[1].at[z], (far * SIDE + y, tp))

    def hidden_units(bufs):
        sz, rz, hz, rs_sems, ag_sems = bufs
        for k in z_steps:
            sent.append((owns(at_z(k)), (sz.at[0], rs_sems[0].at[k])))

        @pl.when(owns(z))
        def _():
            mine = piece_of(z)
            with jax.named_scope("z_reduce"):
                from_z(rz, rs_sems)
            rz[z] = sz[mine]
            both = rz[0].astype(F32)
            for k in range(1, depth):
                both = both + rz[k].astype(F32)
            gate_sum, up_sum = both[0], both[1]
            factor = lax.rsqrt(gate_sum[GROUP : GROUP + 1] / features + EPSILON)
            factor = column(factor, lax.rem(mine, SIDE) * TILE)
            gate_value, up_value = factor * gate_sum, factor * up_sum
            hidden = gate_value / (1.0 + jnp.exp(-gate_value)) * up_value
            hz[mine] = jnp.where(sub < GROUP, hidden, 0.0).astype(BF16)
            for k in z_steps:
                push(hz.at[mine], hz.at[mine], ag_sems[0].at[k], ag_sems[1].at[mine], (at_z(k) * SIDE + y, tp))

        for k in z_steps:
            sent.append((owns(z), (hz.at[0], ag_sems[0].at[k])))
        with jax.named_scope("z_gather"):
            for k in reversed(z_steps):
                far = at_z(k)

                @pl.when(owns(far))
                def _():
                    await_slot(hz.at[piece_of(far)], ag_sems[1].at[piece_of(far)])

        return [
            hz[n * SIDE : (n + 1) * SIDE].astype(F32).reshape(ROWS, LANES).astype(BF16) for n in range(share)
        ]

    to_rows = iota((ROWS, seqs), 0)
    seat = lax.shift_right_logical(to_rows, 3) * GROUP + (to_rows & 7)
    place = jnp.where(((to_rows & 7) < GROUP) & (seat == iota((ROWS, seqs), 1)), 1.0, 0.0).astype(BF16)

    loaded("tokens")
    x = dot(place, tokens[...])
    gain_rows = [jnp.broadcast_to(g[...].astype(F32), (ROWS, width)) for g in (gain_m, gain_b)]
    row_in_tile = iota((ROWS, width), 0) & 7
    with_gains = jnp.where(row_in_tile == GROUP, gain_rows[0], jnp.where(row_in_tile == GROUP + 1, gain_rows[1], x))
    for g in range(SIDE):
        tiles_y[g] = with_gains[g * TILE : (g + 1) * TILE].astype(BF16)
    tiles_all[y] = tiles_y[y]

    scaled = (x * gain_a[...].astype(F32)).astype(BF16)
    squares = jnp.broadcast_to(as_line(row_sum(x * x), 0), (TILE, LANES))
    loaded("gate_a", "up_a")
    for u, weight in enumerate((gate_a, up_a)):
        product = dot(scaled, weight[...])
        for j in range(chunks):
            for g in range(SIDE):
                tile = product[g * TILE : (g + 1) * TILE, j * LANES : (j + 1) * LANES]
                if u == 0:
                    tile = jnp.where(sub == GROUP, squares, tile)
                sy[j // share, (j % share) * SIDE + g, u] = tile.astype(BF16)
    for j in range(chunks, pieces):
        for g in range(SIDE):
            for u in range(2):
                sy[j // share, (j % share) * SIDE + g, u] = jnp.zeros((TILE, LANES), BF16)
        down_a[j] = jnp.zeros((width, LANES), BF16)
        for u in range(2):
            gates_b[j, u] = jnp.zeros((width, LANES), BF16)
        down_b[j] = jnp.zeros((width, LANES), BF16)

    with jax.named_scope("barrier"):
        pl.semaphore_wait(barrier, len(z_steps) + len(plane))

    def portion(ref, which, n):
        return ref.at[which, pl.ds(n * SIDE, SIDE)]

    for n in range(share):
        along_y(lambda far: portion(sy, far, n), lambda near: portion(ry, near, n), [s.at[n] for s in y_sems])
    along_y(lambda far: tiles_y.at[far], lambda near: tiles_all.at[near], tok_sems)
    loaded("down_a")
    along_y(lambda far: down_a.at[pl.ds(far * share, share)], lambda near: down_a_all.at[:, near], down_a_sems)
    down_a_all[:, y] = down_a[pl.ds(y * share, share)]
    loaded("w")
    for u in range(3):
        along_y(lambda far: w_all.at[u, y], lambda near: w_all.at[u, near], [s.at[u] for s in w_sems])
    loaded("wo")
    along_y(lambda far: wo_all.at[y], lambda near: wo_all.at[near], wo_sems)

    sz = ff_a[0]
    for n in range(share):
        with jax.named_scope("y_reduce"):
            from_y(lambda near: portion(ry, near, n), [s.at[n] for s in y_sems])
        rows = pl.ds(n * SIDE, SIDE)
        total = sy[y, rows].astype(F32)
        for k in y_steps:
            total = total + ry[at_y(k), rows].astype(F32)
        sz[rows] = total.astype(BF16)
        send_pieces(ff_a, n)

    loaded("decay")
    spread = jnp.zeros((ROWS, 2 * positions), F32)
    thirds = [split_value(decay[:, h, :], 3) for h in range(2)]
    for n in range(3):
        woven = jnp.zeros((seqs, 2 * positions), F32)
        for h in range(2):
            weave = jnp.where(
                iota((positions, 2 * positions), 1) == 2 * iota((positions, 2 * positions), 0) + h, 1.0, 0.0
            ).astype(BF16)
            woven = woven + dot(thirds[h][n], weave)
        spread = spread + dot(place, woven.astype(BF16))
    from_y(lambda near: tiles_all.at[near], tok_sems)
    own_rows = jnp.zeros((TILE, slab), F32)
    for g in range(SIDE):
        lift = jnp.where(iota((width, slab), 1) == iota((width, slab), 0) + g * width, 1.0, 0.0).astype(BF16)
        own_rows = own_rows + dot(tiles_all[g], lift)
    gain_m_slab, gain_b_slab = own_rows[GROUP : GROUP + 1], own_rows[GROUP + 1 : GROUP + 2]
    wide = iota((TILE, slab), 0) < GROUP
    own_rows = jnp.where(wide, own_rows, 0.0)

    hidden = hidden_units(ff_a)
    from_y(lambda near: down_a_all.at[:, near], down_a_sems)
    partial = jnp.zeros((ROWS, slab), F32)
    for n in range(share):
        partial = partial + dot_rows(hidden[n], down_a_all[n].reshape(slab, LANES))
    send_one, got_one, one_sems = t_one
    for g in range(SIDE):
        send_one[g] = partial[g * TILE : (g + 1) * TILE].astype(BF16)
    got_one[y, tp] = send_one[y]
    over_plane(lambda far: send_one.at[far], got_one, one_sems)
    loaded("gates_b", "down_b")
    with jax.named_scope("plane_one"):
        from_plane(got_one, one_sems)

    def added(ref):
        total = ref[0].astype(F32)
        for k in range(1, tp_count):
            total = total + ref[k].astype(F32)
        return total

    summed = sum((added(got_one.at[g]) for g in range(1, SIDE)), added(got_one.at[0]))
    first_rows = (own_rows + 0.5 * summed).astype(BF16)
    first_all[y] = first_rows

    (
        zq, zkv, qf, sa, ra, rst, za, zst,
        zq_sems, zkv_sems, qf_sems, a_sems, st_sems, za_sems, zst_sems,
    ) = mix_bufs
    inverse = LANES ** (-0.5)
    x = first_rows.astype(F32)
    scaled = (x * gain_m_slab).astype(BF16)
    loaded("forget")
    heads = forget.shape[0]
    r8, c8 = iota((TILE, heads), 0), iota((TILE, heads), 1)
    pick = jnp.where((r8 < 2) & (c8 == 2 * tp + r8), 1.0, 0.0).astype(BF16)
    lines = dot(pick, forget[...])
    side_line = as_line(row_sum(x * x), 0)
    for h in range(2):
        side_line = side_line + as_line(row_sum(scaled.astype(F32) * lines[h : h + 1]), ROWS * (h + 1))
    side_line = jnp.broadcast_to(side_line, (TILE, LANES))
    with jax.named_scope("w_wait"):
        for u in range(3):
            from_y(lambda near: w_all.at[u, near], [s.at[u] for s in w_sems])
    product = [dot(scaled, w_all[u].reshape(slab, 2 * LANES)) for u in range(3)]
    for h in range(2):
        tile = product[0][:, h * LANES : (h + 1) * LANES]
        zq[z, h] = (jnp.where(sub == GROUP, side_line, tile) if h == 0 else tile).astype(BF16)
    along_z(zq, zq_sems)
    for u in range(2):
        for h in range(2):
            zkv[z, 2 * u + h] = product[1 + u][:, h * LANES : (h + 1) * LANES].astype(BF16)
    along_z(zkv, zkv_sems)
    along_y(lambda far: first_all.at[y], lambda near: first_all.at[near], first_sems)
    along_y(
        lambda far: gates_b.at[pl.ds(far * share, share)], lambda near: gates_b_all.at[:, :, near], gates_b_sems
    )
    along_y(lambda far: down_b.at[pl.ds(far * share, share)], lambda near: down_b_all.at[:, near], down_b_sems)
    gates_b_all[:, :, y] = gates_b[pl.ds(y * share, share)]
    down_b_all[:, y] = down_b[pl.ds(y * share, share)]

    with jax.named_scope("z_query"):
        from_z(zq, zq_sems)
    both = zq[0].astype(F32)
    for k in range(1, depth):
        both = both + zq[k].astype(F32)
    line = both[0][GROUP : GROUP + 1]
    factor = column(lax.rsqrt(line / features + EPSILON), 0)
    query = [jnp.where(sub < GROUP, factor * both[h], 0.0).astype(BF16) for h in range(2)]
    for h in range(2):
        qf[y, h] = query[h]
    along_y(lambda far: qf.at[y], lambda near: qf.at[near], qf_sems)
    log_gate = []
    for h in range(2):
        gate = factor * column(line, ROWS * (h + 1)) + bias[2 * tp + h]
        log_gate.append(jnp.minimum(gate, 0.0) - jnp.log(1.0 + jnp.exp(-jnp.abs(gate))))
    loaded("keys", "values")

    with jax.named_scope("y_query"):
        from_y(lambda near: qf.at[near], qf_sems)
    lane2, sub2 = iota((TILE, 2 * positions), 1), iota((TILE, 2 * positions), 0)
    even = lax.rem(lane2, 2) == 0
    stats = jnp.zeros((1, LANES), F32)
    for g in range(SIDE):
        pair = jnp.concatenate([qf[g, 0].astype(F32), qf[g, 1].astype(F32)]).astype(BF16)
        scores = jnp.zeros((TILE, 2 * positions), F32)
        for i in range(GROUP):
            found = dot_rows(pair, keys[g * GROUP + i])
            found = jnp.where(even, found[:TILE], found[TILE:])
            scores = jnp.where(sub2 == i, found, scores)
        scores = scores * inverse + spread[g * TILE : (g + 1) * TILE]
        tops = [
            jnp.max(jnp.where(even if h == 0 else ~even, scores, -jnp.inf), axis=1, keepdims=True)
            for h in range(2)
        ]
        weights = jnp.exp(scores - jnp.where(even, tops[0], tops[1])).astype(BF16).astype(F32)
        parts = [jnp.where(even, weights, 0.0), jnp.where(even, 0.0, weights)]
        sums = [row_sum(part) for part in parts]
        both_parts = jnp.concatenate(parts).astype(BF16)
        mixed = [jnp.zeros((TILE, LANES), F32) for _ in range(2)]
        for i in range(GROUP):
            found = dot(both_parts, values[g * GROUP + i])
            for h in range(2):
                mixed[h] = jnp.where(sub == i, found[h * TILE : (h + 1) * TILE], mixed[h])
        for h in range(2):
            sa[g, h] = (mixed[h] / sums[h]).astype(BF16)
            stats = stats + as_line(tops[h] + jnp.log(sums[h]), ROWS * h + g * TILE)
    rst[y] = stats
    along_y(lambda far: rst.at[y], lambda near: rst.at[near], st_sems)
    along_y(lambda far: sa.at[far], lambda near: ra.at[near], a_sems)
    with jax.named_scope("y_merge"):
        from_y(lambda near: rst.at[near], st_sems)
        from_y(lambda near: ra.at[near], a_sems)

    def merged(levels, parts):
        top = functools.reduce(jnp.maximum, levels)
        shares = [jnp.exp(level - top) for level in levels]
        whole = sum(shares[1:], shares[0])
        value = sum((a * b for a, b in zip(shares[1:], parts[1:])), shares[0] * parts[0])
        return value / whole, top + jnp.log(whole)

    spots = [y] + [at_y(k) for k in y_steps]
    stats = jnp.zeros((1, LANES), F32)
    for h in range(2):
        levels = [column(rst[spot], ROWS * h + y * TILE) for spot in spots]
        parts = [sa[y, h].astype(F32)] + [ra[spot, h].astype(F32) for spot in spots[1:]]
        value, level = merged(levels, parts)
        za[z, h] = value.astype(BF16)
        stats = stats + as_line(level, ROWS * h)
    zst[z] = stats
    along_z(zst, zst_sems)
    along_z(za, za_sems)

    with jax.named_scope("z_keyvalue"):
        from_z(zkv, zkv_sems)
    both = zkv[0].astype(F32)
    for k in range(1, depth):
        both = both + zkv[k].astype(F32)
    fresh = [jnp.where(sub < GROUP, factor * both[u], 0.0).astype(BF16).astype(F32) for u in range(4)]
    own_level = [row_sum(query[h].astype(F32) * fresh[h]) * inverse for h in range(2)]
    from_y(lambda near: first_all.at[near], first_sems)
    from_y(lambda near: gates_b_all.at[:, :, near], gates_b_sems)
    from_y(lambda near: down_b_all.at[:, near], down_b_sems)
    from_y(lambda near: wo_all.at[near], wo_sems)
    with jax.named_scope("z_merge"):
        from_z(zst, zst_sems)
        from_z(za, za_sems)
    attended = []
    for h in range(2):
        levels = [column(zst[k], ROWS * h) + log_gate[h] for k in range(depth)] + [own_level[h]]
        parts = [za[k, h].astype(F32) for k in range(depth)] + [fresh[2 + h]]
        attended.append(merged(levels, parts)[0])
    attended = jnp.concatenate(attended, axis=1).astype(BF16)
    send_two, got_two, two_sems = t_two
    mine = dot_rows(attended, wo_all[...].reshape(slab, 2 * LANES)).astype(BF16)
    send_two[...] = mine
    got_two[y, tp] = mine
    over_plane(lambda far: send_two, got_two, two_sems)
    with jax.named_scope("plane_two"):
        from_plane(got_two, two_sems)

    mixed = jnp.concatenate(
        [(first_all[g].astype(F32) + added(got_two.at[g])).astype(BF16).astype(F32) for g in range(SIDE)]
    )
    scaled = (mixed * gain_b_slab).astype(BF16)
    squares = jnp.broadcast_to(as_line(row_sum(mixed * mixed), 0), (TILE, LANES))
    sz = ff_b[0]
    for n in range(share):
        for u in range(2):
            product = dot(scaled, gates_b_all[n, u].reshape(slab, LANES))
            for g in range(SIDE):
                tile = product[g * TILE : (g + 1) * TILE]
                if u == 0:
                    tile = jnp.where(sub == GROUP, squares, tile)
                sz[n * SIDE + g, u] = tile.astype(BF16)
        send_pieces(ff_b, n)
    lower = jnp.where(iota((slab, width), 0) == iota((slab, width), 1) + y * width, 1.0, 0.0).astype(BF16)
    residual = dot(mixed.astype(BF16), lower)
    hidden = hidden_units(ff_b)
    send_three, got_three, three_sems = t_three
    for g in range(SIDE):
        partial = jnp.zeros((ROWS, width), F32)
        for n in range(share):
            partial = partial + dot_rows(hidden[n], down_b_all[n, g])
        send_three[g] = partial.astype(BF16)
    got_three[y, tp] = send_three[y]
    over_plane(lambda far: send_three.at[far], got_three, three_sems)
    with jax.named_scope("plane_three"):
        from_plane(got_three, three_sems)
    summed = sum((added(got_three.at[g]) for g in range(1, SIDE)), added(got_three.at[0]))
    last = (residual + 0.5 * summed).astype(BF16)

    back = iota((seqs, ROWS), 1)
    seat = lax.shift_right_logical(back, 3) * GROUP + (back & 7)
    lift = jnp.where(((back & 7) < GROUP) & (seat == iota((seqs, ROWS), 0)), 1.0, 0.0).astype(BF16)
    out_ref[...] = dot(lift, last).astype(BF16)

    for condition, copy in sent:
        if condition is None:
            copy.wait_send()
        else:
            ref, sem = copy

            @pl.when(condition)
            def _():
                await_slot(ref, sem)


def on_device(
    ranks,
    tokens,
    gain_first,
    gate_first,
    up_first,
    down_first,
    gain_mixer,
    query_weight,
    key_weight,
    value_weight,
    forget_weight,
    forget_bias,
    key_cache,
    value_cache,
    forget_sum,
    out_weight,
    gain_second,
    gate_second,
    up_second,
    down_second,
):
    kv_count, tp_count = ranks
    depth = kv_count // SIDE
    seqs, length = key_cache.shape[:2]
    chunks = gate_first.shape[1] // LANES
    share = -(-chunks // SIDE)
    pieces = share * SIDE
    width = tokens.shape[1]
    slab = SIDE * width
    dma = pltpu.SemaphoreType.DMA

    def flat(cache):
        return cache.reshape(seqs, 2 * length, LANES)

    operands = [
        tokens,
        gain_first.reshape(1, -1),
        gate_first,
        up_first,
        down_first.T,
        gain_mixer.reshape(1, -1),
        query_weight,
        key_weight,
        value_weight,
        forget_weight.T,
        flat(key_cache),
        flat(value_cache),
        forget_sum,
        out_weight.T,
        gain_second.reshape(1, -1),
        gate_second,
        up_second,
        down_second.T,
    ]

    def half(*dims):
        return pltpu.VMEM(dims, BF16)

    def tiles(*dims):
        return pltpu.VMEM((*dims, TILE, LANES), BF16)

    def pair(count, other=None):
        return (dma((count,)), dma((other or count,)))

    def ff():
        return (tiles(pieces, 2), tiles(depth, 2), tiles(pieces), pair(depth), pair(depth, pieces))

    def plane():
        return (dma((SIDE * tp_count,)), dma((SIDE, tp_count)))

    held = [
        half(seqs, width),
        half(1, width),
        half(*gate_first.shape),
        half(*up_first.shape),
        half(1, width),
        half(1, width),
        half(forget_weight.shape[1], slab),
        half(seqs, 2 * length, LANES),
        half(seqs, 2 * length, LANES),
        pltpu.VMEM(forget_sum.shape, F32),
        half(pieces, width, LANES),
        half(pieces, 2, width, LANES),
        half(pieces, width, LANES),
        half(3, SIDE, width, 2 * LANES),
        half(SIDE, width, 2 * LANES),
        half(share, SIDE, width, LANES),
        half(share, 2, SIDE, width, LANES),
        half(share, SIDE, width, LANES),
        dma((4 + 1 + 1 + chunks + 1 + 3 + 1 + 1 + 1 + 1 + 3 * chunks,)),
        half(SIDE, TILE, width),
        half(SIDE, TILE, width),
        tiles(SIDE, pieces, 2),
        tiles(SIDE, pieces, 2),
        ff(),
        ff(),
        (
            tiles(depth, 2),
            tiles(depth, 4),
            tiles(SIDE, 2),
            tiles(SIDE, 2),
            tiles(SIDE, 2),
            pltpu.VMEM((SIDE, 1, LANES), F32),
            tiles(depth, 2),
            pltpu.VMEM((depth, 1, LANES), F32),
            pair(depth),
            pair(depth),
            pair(SIDE),
            pair(SIDE),
            pair(SIDE),
            pair(depth),
            pair(depth),
        ),
        (half(SIDE, TILE, slab), half(SIDE, tp_count, TILE, slab), plane()),
        (half(TILE, slab), half(SIDE, tp_count, TILE, slab), plane()),
        (half(SIDE, ROWS, width), half(SIDE, tp_count, ROWS, width), plane()),
        half(SIDE, TILE, slab),
        pair(SIDE),
        (dma((share, SIDE)), dma((share, SIDE))),
        pair(SIDE),
        (dma((3, SIDE)), dma((3, SIDE))),
        pair(SIDE),
        pair(SIDE),
        pair(SIDE),
        pair(SIDE),
    ]
    return pl.pallas_call(
        functools.partial(layer_kernel, ranks, width * kv_count),
        out_shape=jax.ShapeDtypeStruct(tokens.shape, BF16),
        in_specs=[pl.BlockSpec(memory_space=pltpu.SMEM)]
        + [pl.BlockSpec(memory_space=pltpu.HBM)] * len(operands),
        out_specs=pl.BlockSpec(memory_space=pltpu.VMEM),
        scratch_shapes=held,
        compiler_params=pltpu.CompilerParams(
            collective_id=0, has_side_effects=True, vmem_limit_bytes=67_043_328
        ),
        name="layer",
    )(forget_bias, *operands)


def solution(mesh):
    ranks = (mesh.shape["kv"], mesh.shape["tp"])
    kv, tp = "kv", "tp"
    in_specs = (
        P(None, kv),
        P(kv),
        P(kv, tp),
        P(kv, tp),
        P(tp, kv),
        P(kv),
        P(kv, tp),
        P(kv, tp),
        P(kv, tp),
        P(),
        P(),
        P(None, kv, tp, None),
        P(None, kv, tp, None),
        P(None, tp, kv),
        P(tp, kv),
        P(kv),
        P(kv, tp),
        P(kv, tp),
        P(tp, kv),
    )
    return jax.shard_map(
        functools.partial(on_device, ranks),
        mesh=mesh,
        in_specs=in_specs,
        out_specs=P(None, kv),
        check_vma=False,
    )
```

```python
import functools

import jax
import jax.numpy as jnp
from jax import lax
from jax.experimental import pallas as pl
from jax.experimental.pallas import tpu as pltpu
from jax.sharding import PartitionSpec as P

MESH = pl.DeviceIdType.MESH
EPSILON = 1e-06
SIDE = 4
GROUP = 6
TILE = 8
ROWS = SIDE * TILE
LANES = 128
F32 = jnp.float32
BF16 = jnp.bfloat16


def dot(left, right):
    return lax.dot_general(left, right, (((1,), (0,)), ((), ())), preferred_element_type=F32)


def dot_rows(left, right):
    return lax.dot_general(left, right, (((1,), (1,)), ((), ())), preferred_element_type=F32)


def iota(shape, dim):
    return lax.broadcasted_iota(jnp.int32, shape, dim)


def far_first(count):
    return sorted(range(1, count), key=lambda k: (-min(k, count - k), k))


def split_value(value, pieces):
    parts = []
    for _ in range(pieces):
        part = value.astype(BF16)
        parts.append(part)
        value = value - part.astype(F32)
    return parts


def layer_kernel(
    ranks,
    features,
    bias_hbm,
    tokens_hbm,
    gain_a_hbm,
    gate_a_hbm,
    up_a_hbm,
    down_a_hbm,
    gain_m_hbm,
    wq_hbm,
    wk_hbm,
    wv_hbm,
    forget_hbm,
    keys_hbm,
    values_hbm,
    decay_hbm,
    wo_hbm,
    gain_b_hbm,
    gate_b_hbm,
    up_b_hbm,
    down_b_hbm,
    out_ref,
    bias,
    tokens,
    gain_a,
    gate_a,
    up_a,
    gain_m,
    gain_b,
    forget,
    keys,
    values,
    decay,
    down_a,
    gates_b,
    down_b,
    w_all,
    wo_all,
    down_a_all,
    gates_b_all,
    down_b_all,
    sems,
    tiles_y,
    tiles_all,
    sy,
    ry,
    ff_a,
    ff_b,
    mix_bufs,
    t_one,
    t_two,
    t_three,
    first_all,
    spread,
):
    kv_count, tp_count = ranks
    depth = kv_count // SIDE
    kv, tp = lax.axis_index("kv"), lax.axis_index("tp")
    z, y = lax.div(kv, SIDE), lax.rem(kv, SIDE)
    chunks = gate_a.shape[1] // LANES
    share = down_a.shape[0] // SIDE
    pieces = share * SIDE
    width = tokens.shape[1]
    slab = SIDE * width
    seqs = tokens.shape[0]
    positions = decay.shape[2]

    def at_z(k):
        return lax.rem(z + k, depth)

    def at_y(k):
        return lax.rem(y + k, SIDE)

    def at_tp(k):
        return lax.rem(tp + k, tp_count)

    z_steps, y_steps = far_first(depth), far_first(SIDE)
    plane = sorted(
        [(a, b) for a in range(SIDE) for b in range(tp_count) if a or b],
        key=lambda s: (-min(s[0], SIDE - s[0]) - min(s[1], tp_count - s[1]) / 2, s),
    )

    counter = iter(range(sems.shape[0]))

    def fresh_sem():
        return sems.at[next(counter)]

    def fresh_pair():
        return fresh_sem(), fresh_sem()

    def take(ref, sem):
        pltpu.make_async_copy(ref, ref, sem).wait()

    barrier = pltpu.get_barrier_semaphore()
    for k in z_steps:
        pl.semaphore_signal(barrier, inc=1, device_id=(at_z(k) * SIDE + y, tp), device_id_type=MESH)

    def columns(ref, j):
        return ref.at[:, pl.ds(j * LANES, LANES)]

    loads = {}

    def load(name, whole, *copies):
        sem = fresh_sem()
        for source, target in copies:
            pltpu.make_async_copy(source, target, sem).start()
        loads[name] = (whole, sem)

    def load_one(name, source, target):
        load(name, target, (source, target))

    def loaded(*names):
        for name in names:
            take(*loads.pop(name))

    load_one("tokens", tokens_hbm, tokens)
    load_one("gain_a", gain_a_hbm, gain_a)
    load_one("gate_a", gate_a_hbm, gate_a)
    load_one("up_a", up_a_hbm, up_a)
    load_one("gain_m", gain_m_hbm, gain_m)
    load_one("gain_b", gain_b_hbm, gain_b)
    for a, b in plane:
        pl.semaphore_signal(barrier, inc=1, device_id=(z * SIDE + at_y(a), at_tp(b)), device_id_type=MESH)
    load("down_a", down_a.at[pl.ds(0, chunks)], *[(columns(down_a_hbm, j), down_a.at[j]) for j in range(chunks)])
    load(
        "w",
        w_all.at[:, y],
        (wq_hbm, w_all.at[0, y]),
        (wk_hbm, w_all.at[1, y]),
        (wv_hbm, w_all.at[2, y]),
    )
    load_one("wo", wo_hbm, wo_all.at[y])
    load_one("decay", decay_hbm, decay)
    load_one("bias", bias_hbm, bias)
    load_one("forget", forget_hbm.at[:, pl.ds(pl.multiple_of(z * slab, slab), slab)], forget)
    load_one("keys", keys_hbm, keys)
    load_one("values", values_hbm, values)
    load(
        "gates_b",
        gates_b.at[pl.ds(0, chunks)],
        *[(columns(gate_b_hbm, j), gates_b.at[j, 0]) for j in range(chunks)],
        *[(columns(up_b_hbm, j), gates_b.at[j, 1]) for j in range(chunks)],
    )
    load("down_b", down_b.at[pl.ds(0, chunks)], *[(columns(down_b_hbm, j), down_b.at[j]) for j in range(chunks)])

    sent = []

    def push(source, target, sems, device):
        pltpu.make_async_remote_copy(
            src_ref=source,
            dst_ref=target,
            send_sem=sems[0],
            recv_sem=sems[1],
            device_id=device,
            device_id_type=MESH,
        ).start()

    def along_y(source_of, target_of, three):
        sems = fresh_pair()
        for k in y_steps:
            far = at_y(k)
            push(source_of(far), target_of(y), sems, (z * SIDE + far, tp))
        sent.append((None, three, sems[0]))
        return lambda: take(three, sems[1])

    def along_z(target):
        sems = fresh_pair()
        for k in z_steps:
            push(target.at[z], target.at[z], sems, (at_z(k) * SIDE + y, tp))
        others = target.at[pl.ds(0, depth - 1)]
        sent.append((None, others, sems[0]))
        return lambda: take(others, sems[1])

    def over_plane(source_of, target):
        sems = fresh_pair()
        for a, b in plane:
            far = at_y(a)
            push(source_of(far), target.at[y * tp_count + tp], sems, (z * SIDE + far, at_tp(b)))
        others = target.at[pl.ds(0, SIDE * tp_count - 1)]
        sent.append((None, others, sems[0]))
        return lambda: take(others, sems[1])

    sub, lane = iota((TILE, LANES), 0), iota((TILE, LANES), 1)

    def column(line, first):
        picked = jnp.where(lane == first + sub, jnp.broadcast_to(line, (TILE, LANES)), 0.0)
        return jnp.sum(picked, axis=1, keepdims=True)

    def as_line(values, first):
        shape = (values.shape[0], LANES)
        spread_out = jnp.where(iota(shape, 1) == first + iota(shape, 0), values, 0.0)
        return jnp.sum(spread_out, axis=0, keepdims=True)

    def row_sum(x):
        return jnp.sum(x, axis=1, keepdims=True)

    def owner(p):
        return lax.div(p * depth, pieces)

    def piece_of(place):
        return lax.div(pieces * place + depth - 1, depth)

    def owns(place):
        p = piece_of(place)
        return jnp.logical_and(p < pieces, owner(p) == place)

    def send_pieces(bufs, sems, n):
        sz, rz, hz = bufs
        for k in z_steps:
            far = at_z(k)
            p = piece_of(far)

            @pl.when(jnp.logical_and(owns(far), lax.div(p, SIDE) == n))
            def _():
                push(sz.at[p], rz.at[z], sems, (far * SIDE + y, tp))

    def hidden_units(bufs, rs_sems):
        sz, rz, hz = bufs
        ag_sems = fresh_pair()
        mine_too = jnp.logical_not(owns(z))
        sent.append((owns(z), sz.at[pl.ds(0, pieces - 1)], rs_sems[0]))
        sent.append((mine_too, sz, rs_sems[0]))

        @pl.when(owns(z))
        def _():
            mine = piece_of(z)
            with jax.named_scope("z_reduce"):
                take(rz.at[pl.ds(0, depth - 1)], rs_sems[1])
            rz[z] = sz[mine]
            both = rz[0].astype(F32)
            for k in range(1, depth):
                both = both + rz[k].astype(F32)
            gate_sum, up_sum = both[0], both[1]
            factor = lax.rsqrt(gate_sum[GROUP : GROUP + 1] / features + EPSILON)
            factor = column(factor, lax.rem(mine, SIDE) * TILE)
            gate_value, up_value = factor * gate_sum, factor * up_sum
            hidden = gate_value / (1.0 + jnp.exp(-gate_value)) * up_value
            hz[mine] = jnp.where(sub < GROUP, hidden, 0.0).astype(BF16)
            for k in z_steps:
                push(hz.at[mine], hz.at[mine], ag_sems, (at_z(k) * SIDE + y, tp))

        sent.append((owns(z), rz.at[pl.ds(0, depth - 1), 0], ag_sems[0]))
        with jax.named_scope("z_gather"):

            @pl.when(owns(z))
            def _():
                take(hz.at[pl.ds(0, pieces - 1)], ag_sems[1])

            @pl.when(mine_too)
            def _():
                take(hz, ag_sems[1])

        return [
            hz[n * SIDE : (n + 1) * SIDE].astype(F32).reshape(ROWS, LANES).astype(BF16) for n in range(share)
        ]

    to_rows = iota((ROWS, seqs), 0)
    seat = lax.shift_right_logical(to_rows, 3) * GROUP + (to_rows & 7)
    place = jnp.where(((to_rows & 7) < GROUP) & (seat == iota((ROWS, seqs), 1)), 1.0, 0.0).astype(BF16)

    loaded("tokens", "gain_a", "gain_m", "gain_b")
    x = dot(place, tokens[...])
    gain_rows = [jnp.broadcast_to(g[...].astype(F32), (ROWS, width)) for g in (gain_m, gain_b)]
    row_in_tile = iota((ROWS, width), 0) & 7
    with_gains = jnp.where(row_in_tile == GROUP, gain_rows[0], jnp.where(row_in_tile == GROUP + 1, gain_rows[1], x))
    for g in range(SIDE):
        tiles_y[g] = with_gains[g * TILE : (g + 1) * TILE].astype(BF16)
    tiles_all[y] = tiles_y[y]

    scaled = (x * gain_a[...].astype(F32)).astype(BF16)
    squares = jnp.broadcast_to(as_line(row_sum(x * x), 0), (TILE, LANES))
    loaded("gate_a", "up_a")
    for u, weight in enumerate((gate_a, up_a)):
        product = dot(scaled, weight[...])
        for j in range(chunks):
            for g in range(SIDE):
                tile = product[g * TILE : (g + 1) * TILE, j * LANES : (j + 1) * LANES]
                if u == 0:
                    tile = jnp.where(sub == GROUP, squares, tile)
                sy[j // share, (j % share) * SIDE + g, u] = tile.astype(BF16)
    for j in range(chunks, pieces):
        for g in range(SIDE):
            for u in range(2):
                sy[j // share, (j % share) * SIDE + g, u] = jnp.zeros((TILE, LANES), BF16)
        down_a[j] = jnp.zeros((width, LANES), BF16)
        for u in range(2):
            gates_b[j, u] = jnp.zeros((width, LANES), BF16)
        down_b[j] = jnp.zeros((width, LANES), BF16)

    with jax.named_scope("barrier"):
        pl.semaphore_wait(barrier, len(z_steps) + len(plane))

    def portion(ref, which, n):
        return ref.at[which, pl.ds(n * SIDE, SIDE)]

    first_three = pl.ds(0, SIDE - 1)
    reduced = [
        along_y(lambda far: portion(sy, far, n), lambda near: portion(ry, near, n), portion(ry, first_three, n))
        for n in range(share)
    ]
    tiles_here = along_y(lambda far: tiles_y.at[far], lambda near: tiles_all.at[near], tiles_all.at[first_three])
    loaded("down_a")
    down_a_here = along_y(
        lambda far: down_a.at[pl.ds(far * share, share)],
        lambda near: down_a_all.at[:, near],
        down_a_all.at[:, first_three],
    )
    down_a_all[:, y] = down_a[pl.ds(y * share, share)]
    loaded("w")
    w_here = along_y(lambda far: w_all.at[:, y], lambda near: w_all.at[:, near], w_all.at[:, first_three])
    loaded("wo")
    wo_here = along_y(lambda far: wo_all.at[y], lambda near: wo_all.at[near], wo_all.at[first_three])

    loaded("down_b")
    down_b_here = along_y(
        lambda far: down_b.at[pl.ds(far * share, share)],
        lambda near: down_b_all.at[:, near],
        down_b_all.at[:, first_three],
    )

    sz, ff_sems = ff_a[0], fresh_pair()
    for n in range(share):
        with jax.named_scope("y_reduce"):
            reduced[n]()
        rows = pl.ds(n * SIDE, SIDE)
        total = sy[y, rows].astype(F32)
        for k in y_steps:
            total = total + ry[at_y(k), rows].astype(F32)
        sz[rows] = total.astype(BF16)
        send_pieces(ff_a, ff_sems, n)

    loaded("decay")
    woven_all = jnp.zeros((ROWS, 2 * positions), F32)
    thirds = [split_value(decay[:, h, :], 3) for h in range(2)]
    for n in range(3):
        woven = jnp.zeros((seqs, 2 * positions), F32)
        for h in range(2):
            weave = jnp.where(
                iota((positions, 2 * positions), 1) == 2 * iota((positions, 2 * positions), 0) + h, 1.0, 0.0
            ).astype(BF16)
            woven = woven + dot(thirds[h][n], weave)
        woven_all = woven_all + dot(place, woven.astype(BF16))
    for g in range(SIDE):
        spread[g] = woven_all[g * TILE : (g + 1) * TILE]
    tiles_here()
    own_rows = jnp.zeros((TILE, slab), F32)
    for g in range(SIDE):
        lift = jnp.where(iota((width, slab), 1) == iota((width, slab), 0) + g * width, 1.0, 0.0).astype(BF16)
        own_rows = own_rows + dot(tiles_all[g], lift)
    gain_m_slab, gain_b_slab = own_rows[GROUP : GROUP + 1], own_rows[GROUP + 1 : GROUP + 2]
    wide = iota((TILE, slab), 0) < GROUP
    own_rows = jnp.where(wide, own_rows, 0.0)

    hidden = hidden_units(ff_a, ff_sems)
    down_a_here()
    partial = jnp.zeros((ROWS, slab), F32)
    for n in range(share):
        partial = partial + dot_rows(hidden[n], down_a_all[n].reshape(slab, LANES))
    send_one, got_one = t_one
    for g in range(SIDE):
        send_one[g] = partial[g * TILE : (g + 1) * TILE].astype(BF16)
    got_one[y * tp_count + tp] = send_one[y]
    one_here = over_plane(lambda far: send_one.at[far], got_one)
    loaded("gates_b")
    with jax.named_scope("plane_one"):
        one_here()

    def added(ref, first, count):
        total = ref[first].astype(F32)
        for k in range(1, count):
            total = total + ref[first + k].astype(F32)
        return total

    summed = added(got_one, 0, SIDE * tp_count)
    first_rows = (own_rows + 0.5 * summed).astype(BF16)
    first_all[y] = first_rows

    zq, zkv, qf, sa, ra, own_stats, rst, za, zst = mix_bufs
    inverse = LANES ** (-0.5)
    x = first_rows.astype(F32)
    scaled = (x * gain_m_slab).astype(BF16)
    loaded("forget", "bias")
    heads = forget.shape[0]
    r8, c8 = iota((TILE, heads), 0), iota((TILE, heads), 1)
    pick = jnp.where((r8 < 2) & (c8 == 2 * tp + r8), 1.0, 0.0).astype(BF16)
    lines = dot(pick, forget[...])
    biases = row_sum(jnp.where((r8 < 2) & (c8 == 2 * tp + r8), jnp.broadcast_to(bias[...], (TILE, heads)), 0.0))
    side_line = as_line(row_sum(x * x), 0)
    for h in range(2):
        side_line = side_line + as_line(row_sum(scaled.astype(F32) * lines[h : h + 1]), ROWS * (h + 1))
    side_line = jnp.broadcast_to(side_line, (TILE, LANES))
    with jax.named_scope("w_wait"):
        w_here()
    product = [dot(scaled, w_all[u].reshape(slab, 2 * LANES)) for u in range(3)]
    for h in range(2):
        tile = product[0][:, h * LANES : (h + 1) * LANES]
        zq[z, h] = (jnp.where(sub == GROUP, side_line, tile) if h == 0 else tile).astype(BF16)
    zq_here = along_z(zq)
    for u in range(2):
        for h in range(2):
            zkv[z, 2 * u + h] = product[1 + u][:, h * LANES : (h + 1) * LANES].astype(BF16)
    first_here = along_y(lambda far: first_all.at[y], lambda near: first_all.at[near], first_all.at[first_three])
    gates_b_here = along_y(
        lambda far: gates_b.at[pl.ds(far * share, share)],
        lambda near: gates_b_all.at[:, :, near],
        gates_b_all.at[:, :, first_three],
    )
    gates_b_all[:, :, y] = gates_b[pl.ds(y * share, share)]
    down_b_all[:, y] = down_b[pl.ds(y * share, share)]

    with jax.named_scope("z_query"):
        zq_here()
    both = zq[0].astype(F32)
    for k in range(1, depth):
        both = both + zq[k].astype(F32)
    line = both[0][GROUP : GROUP + 1]
    factor = column(lax.rsqrt(line / features + EPSILON), 0)
    query = [jnp.where(sub < GROUP, factor * both[h], 0.0).astype(BF16) for h in range(2)]
    for h in range(2):
        qf[y, h] = query[h]
    qf_here = along_y(lambda far: qf.at[y], lambda near: qf.at[near], qf.at[first_three])
    zkv_here = along_z(zkv)
    log_gate = []
    for h in range(2):
        gate = factor * column(line, ROWS * (h + 1)) + biases[h : h + 1]
        log_gate.append(jnp.minimum(gate, 0.0) - jnp.log(1.0 + jnp.exp(-jnp.abs(gate))))
    loaded("keys", "values")

    with jax.named_scope("y_query"):
        qf_here()
    lane2, sub2 = iota((TILE, 2 * positions), 1), iota((TILE, 2 * positions), 0)
    even = lax.rem(lane2, 2) == 0
    ra_sems, rst_sems = fresh_pair(), fresh_pair()
    for k in [*y_steps, 0]:
        g = at_y(k)
        stats = jnp.zeros((1, LANES), F32)
        pair = jnp.concatenate([qf[g, 0].astype(F32), qf[g, 1].astype(F32)]).astype(BF16)
        scores = jnp.zeros((TILE, 2 * positions), F32)
        for i in range(GROUP):
            found = dot_rows(pair, keys[g * GROUP + i])
            found = jnp.where(even, found[:TILE], found[TILE:])
            scores = jnp.where(sub2 == i, found, scores)
        scores = scores * inverse + spread[g]
        tops = [
            jnp.max(jnp.where(even if h == 0 else ~even, scores, -jnp.inf), axis=1, keepdims=True)
            for h in range(2)
        ]
        weights = jnp.exp(scores - jnp.where(even, tops[0], tops[1])).astype(BF16).astype(F32)
        parts = [jnp.where(even, weights, 0.0), jnp.where(even, 0.0, weights)]
        sums = [row_sum(part) for part in parts]
        both_parts = jnp.concatenate(parts).astype(BF16)
        mixed = [jnp.zeros((TILE, LANES), F32) for _ in range(2)]
        for i in range(GROUP):
            found = dot(both_parts, values[g * GROUP + i])
            for h in range(2):
                mixed[h] = jnp.where(sub == i, found[h * TILE : (h + 1) * TILE], mixed[h])
        for h in range(2):
            sa[g, h] = (mixed[h] / sums[h]).astype(BF16)
            stats = stats + as_line(tops[h] + jnp.log(sums[h]), ROWS * h)
        own_stats[g] = stats
        if k:
            push(own_stats.at[g], rst.at[y], rst_sems, (z * SIDE + g, tp))
            push(sa.at[g], ra.at[y], ra_sems, (z * SIDE + g, tp))
    sent.append((None, ra.at[first_three], ra_sems[0]))
    sent.append((None, rst.at[first_three], rst_sems[0]))
    with jax.named_scope("y_merge"):
        take(rst.at[first_three], rst_sems[1])
        take(ra.at[first_three], ra_sems[1])

    def merged(levels, parts):
        top = functools.reduce(jnp.maximum, levels)
        shares = [jnp.exp(level - top) for level in levels]
        whole = sum(shares[1:], shares[0])
        value = sum((a * b for a, b in zip(shares[1:], parts[1:])), shares[0] * parts[0])
        return value / whole, top + jnp.log(whole)

    spots = [y] + [at_y(k) for k in y_steps]
    stats = jnp.zeros((1, LANES), F32)
    for h in range(2):
        levels = [column(own_stats[y], ROWS * h)] + [column(rst[spot], ROWS * h) for spot in spots[1:]]
        parts = [sa[y, h].astype(F32)] + [ra[spot, h].astype(F32) for spot in spots[1:]]
        value, level = merged(levels, parts)
        za[z, h] = value.astype(BF16)
        stats = stats + as_line(level, ROWS * h)
    zst[z] = stats
    zst_here = along_z(zst)
    za_here = along_z(za)

    with jax.named_scope("z_keyvalue"):
        zkv_here()
    both = zkv[0].astype(F32)
    for k in range(1, depth):
        both = both + zkv[k].astype(F32)
    fresh = [jnp.where(sub < GROUP, factor * both[u], 0.0).astype(BF16).astype(F32) for u in range(4)]
    own_level = [row_sum(query[h].astype(F32) * fresh[h]) * inverse for h in range(2)]
    first_here()
    gates_b_here()
    down_b_here()
    wo_here()
    with jax.named_scope("z_merge"):
        zst_here()
        za_here()
    attended = []
    for h in range(2):
        levels = [column(zst[k], ROWS * h) + log_gate[h] for k in range(depth)] + [own_level[h]]
        parts = [za[k, h].astype(F32) for k in range(depth)] + [fresh[2 + h]]
        attended.append(merged(levels, parts)[0])
    attended = jnp.concatenate(attended, axis=1).astype(BF16)
    send_two, got_two = t_two
    mine = dot_rows(attended, wo_all[...].reshape(slab, 2 * LANES)).astype(BF16)
    send_two[...] = mine
    got_two[y * tp_count + tp] = mine
    two_here = over_plane(lambda far: send_two, got_two)
    with jax.named_scope("plane_two"):
        two_here()

    mixed = jnp.concatenate(
        [(first_all[g].astype(F32) + added(got_two, g * tp_count, tp_count)).astype(BF16).astype(F32) for g in range(SIDE)]
    )
    scaled = (mixed * gain_b_slab).astype(BF16)
    squares = jnp.broadcast_to(as_line(row_sum(mixed * mixed), 0), (TILE, LANES))
    sz, ff_sems = ff_b[0], fresh_pair()
    for n in range(share):
        for u in range(2):
            product = dot(scaled, gates_b_all[n, u].reshape(slab, LANES))
            for g in range(SIDE):
                tile = product[g * TILE : (g + 1) * TILE]
                if u == 0:
                    tile = jnp.where(sub == GROUP, squares, tile)
                sz[n * SIDE + g, u] = tile.astype(BF16)
        send_pieces(ff_b, ff_sems, n)
    lower = jnp.where(iota((slab, width), 0) == iota((slab, width), 1) + y * width, 1.0, 0.0).astype(BF16)
    residual = dot(mixed.astype(BF16), lower)
    hidden = hidden_units(ff_b, ff_sems)
    send_three, got_three = t_three
    for g in range(SIDE):
        partial = jnp.zeros((ROWS, width), F32)
        for n in range(share):
            partial = partial + dot_rows(hidden[n], down_b_all[n, g])
        send_three[g] = partial.astype(BF16)
    got_three[y * tp_count + tp] = send_three[y]
    three_here = over_plane(lambda far: send_three.at[far], got_three)
    with jax.named_scope("plane_three"):
        three_here()
    summed = added(got_three, 0, SIDE * tp_count)
    last = (residual + 0.5 * summed).astype(BF16)

    back = iota((seqs, ROWS), 1)
    seat = lax.shift_right_logical(back, 3) * GROUP + (back & 7)
    lift = jnp.where(((back & 7) < GROUP) & (seat == iota((seqs, ROWS), 0)), 1.0, 0.0).astype(BF16)
    out_ref[...] = dot(lift, last).astype(BF16)

    for condition, ref, sem in sent:
        if condition is None:
            take(ref, sem)
        else:

            @pl.when(condition)
            def _():
                take(ref, sem)


def on_device(
    ranks,
    tokens,
    gain_first,
    gate_first,
    up_first,
    down_first,
    gain_mixer,
    query_weight,
    key_weight,
    value_weight,
    forget_weight,
    forget_bias,
    key_cache,
    value_cache,
    forget_sum,
    out_weight,
    gain_second,
    gate_second,
    up_second,
    down_second,
):
    kv_count, tp_count = ranks
    depth = kv_count // SIDE
    seqs, length = key_cache.shape[:2]
    chunks = gate_first.shape[1] // LANES
    share = -(-chunks // SIDE)
    pieces = share * SIDE
    width = tokens.shape[1]
    slab = SIDE * width
    dma = pltpu.SemaphoreType.DMA

    def flat(cache):
        return cache.reshape(seqs, 2 * length, LANES)

    operands = [
        tokens,
        gain_first.reshape(1, -1),
        gate_first,
        up_first,
        down_first.T,
        gain_mixer.reshape(1, -1),
        query_weight,
        key_weight,
        value_weight,
        forget_weight.T,
        flat(key_cache),
        flat(value_cache),
        forget_sum,
        out_weight.T,
        gain_second.reshape(1, -1),
        gate_second,
        up_second,
        down_second.T,
    ]

    def half(*dims):
        return pltpu.VMEM(dims, BF16)

    def tiles(*dims):
        return pltpu.VMEM((*dims, TILE, LANES), BF16)

    def ff():
        return (tiles(pieces, 2), tiles(depth, 2), tiles(pieces))

    held = [
        pltpu.VMEM((1, forget_weight.shape[1]), F32),
        half(seqs, width),
        half(1, width),
        half(*gate_first.shape),
        half(*up_first.shape),
        half(1, width),
        half(1, width),
        half(forget_weight.shape[1], slab),
        half(seqs, 2 * length, LANES),
        half(seqs, 2 * length, LANES),
        pltpu.VMEM(forget_sum.shape, F32),
        half(pieces, width, LANES),
        half(pieces, 2, width, LANES),
        half(pieces, width, LANES),
        half(3, SIDE, width, 2 * LANES),
        half(SIDE, width, 2 * LANES),
        half(share, SIDE, width, LANES),
        half(share, 2, SIDE, width, LANES),
        half(share, SIDE, width, LANES),
        dma((16 + 2 * (share + 21),)),
        half(SIDE, TILE, width),
        half(SIDE, TILE, width),
        tiles(SIDE, pieces, 2),
        tiles(SIDE, pieces, 2),
        ff(),
        ff(),
        (
            tiles(depth, 2),
            tiles(depth, 4),
            tiles(SIDE, 2),
            tiles(SIDE, 2),
            tiles(SIDE, 2),
            pltpu.VMEM((SIDE, 1, LANES), F32),
            pltpu.VMEM((SIDE, 1, LANES), F32),
            tiles(depth, 2),
            pltpu.VMEM((depth, 1, LANES), F32),
        ),
        (half(SIDE, TILE, slab), half(SIDE * tp_count, TILE, slab)),
        (half(TILE, slab), half(SIDE * tp_count, TILE, slab)),
        (half(SIDE, ROWS, width), half(SIDE * tp_count, ROWS, width)),
        half(SIDE, TILE, slab),
        pltpu.VMEM((SIDE, TILE, 2 * length), F32),
    ]
    return pl.pallas_call(
        functools.partial(layer_kernel, ranks, width * kv_count),
        out_shape=jax.ShapeDtypeStruct(tokens.shape, BF16),
        in_specs=[pl.BlockSpec(memory_space=pltpu.HBM)] * (1 + len(operands)),
        out_specs=pl.BlockSpec(memory_space=pltpu.VMEM),
        scratch_shapes=held,
        compiler_params=pltpu.CompilerParams(
            collective_id=0, has_side_effects=True, vmem_limit_bytes=67_043_328
        ),
        name="layer",
    )(forget_bias.reshape(1, -1), *operands)


def solution(mesh):
    ranks = (mesh.shape["kv"], mesh.shape["tp"])
    kv, tp = "kv", "tp"
    in_specs = (
        P(None, kv),
        P(kv),
        P(kv, tp),
        P(kv, tp),
        P(tp, kv),
        P(kv),
        P(kv, tp),
        P(kv, tp),
        P(kv, tp),
        P(),
        P(),
        P(None, kv, tp, None),
        P(None, kv, tp, None),
        P(None, tp, kv),
        P(tp, kv),
        P(kv),
        P(kv, tp),
        P(kv, tp),
        P(tp, kv),
    )
    return jax.shard_map(
        functools.partial(on_device, ranks),
        mesh=mesh,
        in_specs=in_specs,
        out_specs=P(None, kv),
        check_vma=False,
    )
```

```python
import functools

import jax
import jax.numpy as jnp
from jax import lax
from jax.experimental import pallas as pl
from jax.experimental.pallas import tpu as pltpu
from jax.sharding import PartitionSpec as P

MESH = pl.DeviceIdType.MESH
EPSILON = 1e-06
SIDE = 4
GROUP = 6
TILE = 8
ROWS = SIDE * TILE
LANES = 128
F32 = jnp.float32
BF16 = jnp.bfloat16


def dot(left, right):
    return lax.dot_general(left, right, (((1,), (0,)), ((), ())), preferred_element_type=F32)


def dot_rows(left, right):
    return lax.dot_general(left, right, (((1,), (1,)), ((), ())), preferred_element_type=F32)


def iota(shape, dim):
    return lax.broadcasted_iota(jnp.int32, shape, dim)


def far_first(count):
    return sorted(range(1, count), key=lambda k: (-min(k, count - k), k))


def split_value(value, pieces):
    parts = []
    for _ in range(pieces):
        part = value.astype(BF16)
        parts.append(part)
        value = value - part.astype(F32)
    return parts


def layer_kernel(
    ranks,
    features,
    bias_hbm,
    tokens_hbm,
    gain_a_hbm,
    gate_a_hbm,
    up_a_hbm,
    down_a_hbm,
    gain_m_hbm,
    wq_hbm,
    wk_hbm,
    wv_hbm,
    forget_hbm,
    keys_hbm,
    values_hbm,
    decay_hbm,
    wo_hbm,
    gain_b_hbm,
    gate_b_hbm,
    up_b_hbm,
    down_b_hbm,
    out_ref,
    bias,
    tokens,
    gain_a,
    gate_a,
    up_a,
    gain_m,
    gain_b,
    forget,
    keys,
    values,
    decay,
    down_a,
    gates_b,
    down_b,
    w_all,
    wo_all,
    down_a_all,
    gates_b_all,
    down_b_all,
    sems,
    entry_sems,
    out_tile,
    tiles_y,
    tiles_all,
    sy,
    ry,
    ff_a,
    ff_b,
    mix_bufs,
    t_one,
    t_two,
    t_three,
    first_all,
    spread,
):
    kv_count, tp_count = ranks
    depth = kv_count // SIDE
    kv, tp = lax.axis_index("kv"), lax.axis_index("tp")
    z, y = lax.div(kv, SIDE), lax.rem(kv, SIDE)
    chunks = gate_a.shape[1] // LANES
    share = down_a.shape[0] // SIDE
    pieces = share * SIDE
    width = tokens.shape[1]
    slab = SIDE * width
    seqs = tokens.shape[0]
    positions = decay.shape[2]

    def at_z(k):
        return lax.rem(z + k, depth)

    def at_y(k):
        return lax.rem(y + k, SIDE)

    def at_tp(k):
        return lax.rem(tp + k, tp_count)

    z_steps, y_steps = far_first(depth), far_first(SIDE)
    plane = sorted(
        [(a, b) for a in range(SIDE) for b in range(tp_count) if a or b],
        key=lambda s: (-min(s[0], SIDE - s[0]) - min(s[1], tp_count - s[1]) / 2, s),
    )

    counter = iter(range(sems.shape[0]))

    def fresh_sem():
        return sems.at[next(counter)]

    def fresh_pair():
        return fresh_sem(), fresh_sem()

    def take(ref, sem):
        pltpu.make_async_copy(ref, ref, sem).wait()

    barrier = pltpu.get_barrier_semaphore()
    near_sem, far_sem = entry_sems

    def signal(sem, device):
        pl.semaphore_signal(sem, inc=1, device_id=device, device_id_type=MESH)

    for k in z_steps:
        signal(barrier, (at_z(k) * SIDE, tp))
    for k in y_steps:

        @pl.when(at_y(k) != 0)
        def _():
            signal(barrier, (z * SIDE + at_y(k), tp))

    def columns(ref, j):
        return ref.at[:, pl.ds(j * LANES, LANES)]

    loads = {}

    def load(name, whole, *copies):
        sem = fresh_sem()
        for source, target in copies:
            pltpu.make_async_copy(source, target, sem).start()
        loads[name] = (whole, sem)

    def load_one(name, source, target):
        load(name, target, (source, target))

    def loaded(*names):
        for name in names:
            take(*loads.pop(name))

    load_one("tokens", tokens_hbm, tokens)
    load_one("gain_a", gain_a_hbm, gain_a)
    load_one("gate_a", gate_a_hbm, gate_a)
    load_one("up_a", up_a_hbm, up_a)
    load_one("gain_m", gain_m_hbm, gain_m)
    load_one("gain_b", gain_b_hbm, gain_b)
    for k in far_first(tp_count):
        signal(barrier, (z * SIDE, at_tp(k)))
    load("down_a", down_a.at[pl.ds(0, chunks)], *[(columns(down_a_hbm, j), down_a.at[j]) for j in range(chunks)])
    load(
        "w",
        w_all.at[:, y],
        (wq_hbm, w_all.at[0, y]),
        (wk_hbm, w_all.at[1, y]),
        (wv_hbm, w_all.at[2, y]),
    )
    load_one("wo", wo_hbm, wo_all.at[y])
    load_one("decay", decay_hbm, decay)
    load_one("bias", bias_hbm, bias)
    load_one("forget", forget_hbm.at[:, pl.ds(pl.multiple_of(z * slab, slab), slab)], forget)
    load_one("keys", keys_hbm, keys)
    load_one("values", values_hbm, values)
    load(
        "gates_b",
        gates_b.at[pl.ds(0, chunks)],
        *[(columns(gate_b_hbm, j), gates_b.at[j, 0]) for j in range(chunks)],
        *[(columns(up_b_hbm, j), gates_b.at[j, 1]) for j in range(chunks)],
    )
    load("down_b", down_b.at[pl.ds(0, chunks)], *[(columns(down_b_hbm, j), down_b.at[j]) for j in range(chunks)])

    sent = []

    def push(source, target, sems, device):
        pltpu.make_async_remote_copy(
            src_ref=source,
            dst_ref=target,
            send_sem=sems[0],
            recv_sem=sems[1],
            device_id=device,
            device_id_type=MESH,
        ).start()

    filled = pl.ds(0, GROUP)

    def rows_of(ref, which):
        return ref.at[which, :, filled]

    def along_y(source_of, target_of, three):
        sems = fresh_pair()
        for k in y_steps:
            far = at_y(k)
            push(source_of(far), target_of(y), sems, (z * SIDE + far, tp))
        sent.append((None, three, sems[0]))
        return lambda: take(three, sems[1])

    def along_z(target, view=lambda ref, which: ref.at[which]):
        sems = fresh_pair()
        for k in z_steps:
            push(view(target, z), view(target, z), sems, (at_z(k) * SIDE + y, tp))
        others = view(target, pl.ds(0, depth - 1))
        sent.append((None, others, sems[0]))
        return lambda: take(others, sems[1])

    def over_plane(source_of, target, view):
        sems = fresh_pair()
        for a, b in plane:
            far = at_y(a)
            push(source_of(far), view(target, y * tp_count + tp), sems, (z * SIDE + far, at_tp(b)))
        others = view(target, pl.ds(0, SIDE * tp_count - 1))
        sent.append((None, others, sems[0]))
        return lambda: take(others, sems[1])

    sub, lane = iota((TILE, LANES), 0), iota((TILE, LANES), 1)

    def column(line, first):
        picked = jnp.where(lane == first + sub, jnp.broadcast_to(line, (TILE, LANES)), 0.0)
        return jnp.sum(picked, axis=1, keepdims=True)

    def as_line(values, first):
        shape = (values.shape[0], LANES)
        spread_out = jnp.where(iota(shape, 1) == first + iota(shape, 0), values, 0.0)
        return jnp.sum(spread_out, axis=0, keepdims=True)

    def row_sum(x):
        return jnp.sum(x, axis=1, keepdims=True)

    def owner(p):
        return lax.div(p * depth, pieces)

    def piece_of(place):
        return lax.div(pieces * place + depth - 1, depth)

    def owns(place):
        p = piece_of(place)
        return jnp.logical_and(p < pieces, owner(p) == place)

    def send_pieces(bufs, sems, n):
        sz, rz, hz = bufs
        for k in z_steps:
            far = at_z(k)
            p = piece_of(far)

            @pl.when(jnp.logical_and(owns(far), lax.div(p, SIDE) == n))
            def _():
                push(sz.at[p], rz.at[z], sems, (far * SIDE + y, tp))

    def hidden_units(bufs, rs_sems):
        sz, rz, hz = bufs
        ag_sems = fresh_pair()
        mine_too = jnp.logical_not(owns(z))
        sent.append((owns(z), sz.at[pl.ds(0, pieces - 1)], rs_sems[0]))
        sent.append((mine_too, sz, rs_sems[0]))

        @pl.when(owns(z))
        def _():
            mine = piece_of(z)
            with jax.named_scope("z_reduce"):
                take(rz.at[pl.ds(0, depth - 1)], rs_sems[1])
            rz[z] = sz[mine]
            both = rz[0].astype(F32)
            for k in range(1, depth):
                both = both + rz[k].astype(F32)
            gate_sum, up_sum = both[0], both[1]
            factor = lax.rsqrt(gate_sum[GROUP : GROUP + 1] / features + EPSILON)
            factor = column(factor, lax.rem(mine, SIDE) * TILE)
            gate_value, up_value = factor * gate_sum, factor * up_sum
            hidden = gate_value / (1.0 + jnp.exp(-gate_value)) * up_value
            hz[mine] = jnp.where(sub < GROUP, hidden, 0.0).astype(BF16)
            for k in z_steps:
                push(hz.at[mine, filled], hz.at[mine, filled], ag_sems, (at_z(k) * SIDE + y, tp))

        sent.append((owns(z), rz.at[pl.ds(0, depth - 1), 0, filled], ag_sems[0]))
        with jax.named_scope("z_gather"):

            @pl.when(owns(z))
            def _():
                take(hz.at[pl.ds(0, pieces - 1), filled], ag_sems[1])

            @pl.when(mine_too)
            def _():
                take(hz.at[:, filled], ag_sems[1])

        return [
            hz[n * SIDE : (n + 1) * SIDE].astype(F32).reshape(ROWS, LANES).astype(BF16) for n in range(share)
        ]

    to_rows = iota((ROWS, seqs), 0)
    seat = lax.shift_right_logical(to_rows, 3) * GROUP + (to_rows & 7)
    place = jnp.where(((to_rows & 7) < GROUP) & (seat == iota((ROWS, seqs), 1)), 1.0, 0.0).astype(BF16)

    loaded("tokens", "gain_a", "gain_m", "gain_b")
    x = dot(place, tokens[...])
    gain_rows = [jnp.broadcast_to(g[...].astype(F32), (ROWS, width)) for g in (gain_m, gain_b)]
    row_in_tile = iota((ROWS, width), 0) & 7
    with_gains = jnp.where(row_in_tile == GROUP, gain_rows[0], jnp.where(row_in_tile == GROUP + 1, gain_rows[1], x))
    for g in range(SIDE):
        tiles_y[g] = with_gains[g * TILE : (g + 1) * TILE].astype(BF16)
    tiles_all[y] = tiles_y[y]

    scaled = (x * gain_a[...].astype(F32)).astype(BF16)
    squares = jnp.broadcast_to(as_line(row_sum(x * x), 0), (TILE, LANES))
    loaded("gate_a", "up_a")
    for u, weight in enumerate((gate_a, up_a)):
        product = dot(scaled, weight[...])
        for j in range(chunks):
            for g in range(SIDE):
                tile = product[g * TILE : (g + 1) * TILE, j * LANES : (j + 1) * LANES]
                if u == 0:
                    tile = jnp.where(sub == GROUP, squares, tile)
                sy[j // share, (j % share) * SIDE + g, u] = tile.astype(BF16)
    for j in range(chunks, pieces):
        for g in range(SIDE):
            for u in range(2):
                sy[j // share, (j % share) * SIDE + g, u] = jnp.zeros((TILE, LANES), BF16)
        down_a[j] = jnp.zeros((width, LANES), BF16)
        for u in range(2):
            gates_b[j, u] = jnp.zeros((width, LANES), BF16)
        down_b[j] = jnp.zeros((width, LANES), BF16)

    with jax.named_scope("barrier"):

        @pl.when(y != 0)
        def _():
            pl.semaphore_wait(barrier, len(y_steps))
            signal(near_sem, (z * SIDE, tp))

        @pl.when(y == 0)
        def _():
            pl.semaphore_wait(near_sem, len(y_steps))


    def portion(ref, which, n):
        return ref.at[which, pl.ds(n * SIDE, SIDE), :, pl.ds(0, GROUP if n else TILE)]

    first_three = pl.ds(0, SIDE - 1)
    reduced = [
        along_y(lambda far: portion(sy, far, n), lambda near: portion(ry, near, n), portion(ry, first_three, n))
        for n in range(share)
    ]
    tiles_here = along_y(lambda far: tiles_y.at[far], lambda near: tiles_all.at[near], tiles_all.at[first_three])
    loaded("down_a")
    down_a_here = along_y(
        lambda far: down_a.at[pl.ds(far * share, share)],
        lambda near: down_a_all.at[:, near],
        down_a_all.at[:, first_three],
    )
    down_a_all[:, y] = down_a[pl.ds(y * share, share)]
    loaded("w")
    w_here = along_y(lambda far: w_all.at[:, y], lambda near: w_all.at[:, near], w_all.at[:, first_three])
    loaded("wo")
    wo_here = along_y(lambda far: wo_all.at[y], lambda near: wo_all.at[near], wo_all.at[first_three])

    loaded("down_b")
    down_b_here = along_y(
        lambda far: down_b.at[pl.ds(far * share, share)],
        lambda near: down_b_all.at[:, near],
        down_b_all.at[:, first_three],
    )

    sz, ff_sems = ff_a[0], fresh_pair()
    for n in range(share):
        with jax.named_scope("y_reduce"):
            reduced[n]()
        rows = pl.ds(n * SIDE, SIDE)
        total = sy[y, rows].astype(F32)
        for k in y_steps:
            total = total + ry[at_y(k), rows].astype(F32)
        if n == 0:
            line = total[0, 0, GROUP : GROUP + 1]
        gates = jnp.where(sub == GROUP, jnp.broadcast_to(line, (TILE, LANES)), total[:, 0])
        sz[rows, 0] = gates.astype(BF16)
        sz[rows, 1] = total[:, 1].astype(BF16)
        if n == 0:
            with jax.named_scope("barrier_far"):

                @pl.when(y == 0)
                def _():
                    pl.semaphore_wait(barrier, SIDE * (len(z_steps) + tp_count - 1))
                    for k in y_steps:
                        signal(far_sem, (z * SIDE + at_y(k), tp))

                @pl.when(y != 0)
                def _():
                    pl.semaphore_wait(far_sem, 1)

        send_pieces(ff_a, ff_sems, n)

    loaded("decay")
    woven_all = jnp.zeros((ROWS, 2 * positions), F32)
    thirds = [split_value(decay[:, h, :], 3) for h in range(2)]
    for n in range(3):
        woven = jnp.zeros((seqs, 2 * positions), F32)
        for h in range(2):
            weave = jnp.where(
                iota((positions, 2 * positions), 1) == 2 * iota((positions, 2 * positions), 0) + h, 1.0, 0.0
            ).astype(BF16)
            woven = woven + dot(thirds[h][n], weave)
        woven_all = woven_all + dot(place, woven.astype(BF16))
    for g in range(SIDE):
        spread[g] = woven_all[g * TILE : (g + 1) * TILE]
    tiles_here()
    own_rows = jnp.zeros((TILE, slab), F32)
    for g in range(SIDE):
        lift = jnp.where(iota((width, slab), 1) == iota((width, slab), 0) + g * width, 1.0, 0.0).astype(BF16)
        own_rows = own_rows + dot(tiles_all[g], lift)
    gain_m_slab, gain_b_slab = own_rows[GROUP : GROUP + 1], own_rows[GROUP + 1 : GROUP + 2]
    wide = iota((TILE, slab), 0) < GROUP
    own_rows = jnp.where(wide, own_rows, 0.0)

    hidden = hidden_units(ff_a, ff_sems)
    down_a_here()
    partial = jnp.zeros((ROWS, slab), F32)
    for n in range(share):
        partial = partial + dot_rows(hidden[n], down_a_all[n].reshape(slab, LANES))
    send_one, got_one = t_one
    for g in range(SIDE):
        send_one[g] = partial[g * TILE : (g + 1) * TILE].astype(BF16)
    got_one[y * tp_count + tp] = send_one[y]
    one_here = over_plane(lambda far: send_one.at[far, filled], got_one, lambda ref, which: ref.at[which, filled])
    loaded("gates_b")
    with jax.named_scope("plane_one"):
        one_here()

    def added(ref, first, count):
        total = ref[first].astype(F32)
        for k in range(1, count):
            total = total + ref[first + k].astype(F32)
        return total

    summed = added(got_one, 0, SIDE * tp_count)
    first_rows = (own_rows + 0.5 * summed).astype(BF16)
    first_all[y] = first_rows

    zq, zkv, qf, sa, ra, own_stats, rst, za, zst = mix_bufs
    inverse = LANES ** (-0.5)
    x = first_rows.astype(F32)
    scaled = (x * gain_m_slab).astype(BF16)
    loaded("forget", "bias")
    heads = forget.shape[0]
    r8, c8 = iota((TILE, heads), 0), iota((TILE, heads), 1)
    pick = jnp.where((r8 < 2) & (c8 == 2 * tp + r8), 1.0, 0.0).astype(BF16)
    lines = dot(pick, forget[...])
    biases = row_sum(jnp.where((r8 < 2) & (c8 == 2 * tp + r8), jnp.broadcast_to(bias[...], (TILE, heads)), 0.0))
    side_line = as_line(row_sum(x * x), 0)
    for h in range(2):
        side_line = side_line + as_line(row_sum(scaled.astype(F32) * lines[h : h + 1]), ROWS * (h + 1))
    side_line = jnp.broadcast_to(side_line, (TILE, LANES))
    with jax.named_scope("w_wait"):
        w_here()
    product = [dot(scaled, w_all[u].reshape(slab, 2 * LANES)) for u in range(3)]
    for h in range(2):
        tile = product[0][:, h * LANES : (h + 1) * LANES]
        zq[z, h] = (jnp.where(sub == GROUP, side_line, tile) if h == 0 else tile).astype(BF16)
    zq_here = along_z(zq)
    for u in range(2):
        for h in range(2):
            zkv[z, 2 * u + h] = product[1 + u][:, h * LANES : (h + 1) * LANES].astype(BF16)
    first_here = along_y(
        lambda far: first_all.at[y, filled],
        lambda near: first_all.at[near, filled],
        first_all.at[first_three, filled],
    )
    gates_b_here = along_y(
        lambda far: gates_b.at[pl.ds(far * share, share)],
        lambda near: gates_b_all.at[:, :, near],
        gates_b_all.at[:, :, first_three],
    )
    gates_b_all[:, :, y] = gates_b[pl.ds(y * share, share)]
    down_b_all[:, y] = down_b[pl.ds(y * share, share)]

    with jax.named_scope("z_query"):
        zq_here()
    both = zq[0].astype(F32)
    for k in range(1, depth):
        both = both + zq[k].astype(F32)
    line = both[0][GROUP : GROUP + 1]
    factor = column(lax.rsqrt(line / features + EPSILON), 0)
    query = [jnp.where(sub < GROUP, factor * both[h], 0.0).astype(BF16) for h in range(2)]
    for h in range(2):
        qf[y, h] = query[h]
    qf_here = along_y(lambda far: rows_of(qf, y), lambda near: rows_of(qf, near), rows_of(qf, first_three))
    zkv_here = along_z(zkv, rows_of)
    log_gate = []
    for h in range(2):
        gate = factor * column(line, ROWS * (h + 1)) + biases[h : h + 1]
        log_gate.append(jnp.minimum(gate, 0.0) - jnp.log(1.0 + jnp.exp(-jnp.abs(gate))))
    loaded("keys", "values")

    with jax.named_scope("y_query"):
        qf_here()
    lane2, sub2 = iota((TILE, 2 * positions), 1), iota((TILE, 2 * positions), 0)
    even = lax.rem(lane2, 2) == 0
    ra_sems, rst_sems = fresh_pair(), fresh_pair()
    for k in [*y_steps, 0]:
        g = at_y(k)
        stats = jnp.zeros((1, LANES), F32)
        pair = jnp.concatenate([jnp.where(sub < GROUP, qf[g, h].astype(F32), 0.0) for h in range(2)]).astype(BF16)
        scores = jnp.zeros((TILE, 2 * positions), F32)
        for i in range(GROUP):
            found = dot_rows(pair, keys[g * GROUP + i])
            found = jnp.where(even, found[:TILE], found[TILE:])
            scores = jnp.where(sub2 == i, found, scores)
        scores = scores * inverse + spread[g]
        tops = [
            jnp.max(jnp.where(even if h == 0 else ~even, scores, -jnp.inf), axis=1, keepdims=True)
            for h in range(2)
        ]
        weights = jnp.exp(scores - jnp.where(even, tops[0], tops[1])).astype(BF16).astype(F32)
        parts = [jnp.where(even, weights, 0.0), jnp.where(even, 0.0, weights)]
        sums = [row_sum(part) for part in parts]
        both_parts = jnp.concatenate(parts).astype(BF16)
        mixed = [jnp.zeros((TILE, LANES), F32) for _ in range(2)]
        for i in range(GROUP):
            found = dot(both_parts, values[g * GROUP + i])
            for h in range(2):
                mixed[h] = jnp.where(sub == i, found[h * TILE : (h + 1) * TILE], mixed[h])
        for h in range(2):
            sa[g, h] = (mixed[h] / sums[h]).astype(BF16)
            stats = stats + as_line(tops[h] + jnp.log(sums[h]), ROWS * h)
        own_stats[g] = stats
        if k:
            push(own_stats.at[g], rst.at[y], rst_sems, (z * SIDE + g, tp))
            push(rows_of(sa, g), rows_of(ra, y), ra_sems, (z * SIDE + g, tp))
    sent.append((None, rows_of(ra, first_three), ra_sems[0]))
    sent.append((None, rst.at[first_three], rst_sems[0]))
    with jax.named_scope("y_merge"):
        take(rst.at[first_three], rst_sems[1])
        take(rows_of(ra, first_three), ra_sems[1])

    def merged(levels, parts):
        top = functools.reduce(jnp.maximum, levels)
        shares = [jnp.exp(level - top) for level in levels]
        whole = sum(shares[1:], shares[0])
        value = sum((a * b for a, b in zip(shares[1:], parts[1:])), shares[0] * parts[0])
        return value / whole, top + jnp.log(whole)

    spots = [y] + [at_y(k) for k in y_steps]
    stats = jnp.zeros((1, LANES), F32)
    for h in range(2):
        levels = [column(own_stats[y], ROWS * h)] + [column(rst[spot], ROWS * h) for spot in spots[1:]]
        parts = [sa[y, h].astype(F32)] + [ra[spot, h].astype(F32) for spot in spots[1:]]
        value, level = merged(levels, parts)
        za[z, h] = value.astype(BF16)
        stats = stats + as_line(level, ROWS * h)
    zst[z] = stats
    zst_here = along_z(zst)
    za_here = along_z(za, rows_of)

    with jax.named_scope("z_keyvalue"):
        zkv_here()
    both = zkv[0].astype(F32)
    for k in range(1, depth):
        both = both + zkv[k].astype(F32)
    fresh = [jnp.where(sub < GROUP, factor * both[u], 0.0).astype(BF16).astype(F32) for u in range(4)]
    own_level = [row_sum(query[h].astype(F32) * fresh[h]) * inverse for h in range(2)]
    first_here()
    gates_b_here()
    down_b_here()
    wo_here()
    with jax.named_scope("z_merge"):
        zst_here()
        za_here()
    attended = []
    for h in range(2):
        levels = [column(zst[k], ROWS * h) + log_gate[h] for k in range(depth)] + [own_level[h]]
        parts = [za[k, h].astype(F32) for k in range(depth)] + [fresh[2 + h]]
        attended.append(merged(levels, parts)[0])
    attended = jnp.concatenate(attended, axis=1).astype(BF16)
    send_two, got_two = t_two
    mine = dot_rows(attended, wo_all[...].reshape(slab, 2 * LANES)).astype(BF16)
    send_two[...] = mine
    got_two[y * tp_count + tp] = mine
    two_here = over_plane(lambda far: send_two.at[filled], got_two, lambda ref, which: ref.at[which, filled])
    with jax.named_scope("plane_two"):
        two_here()

    mixed = jnp.concatenate(
        [(first_all[g].astype(F32) + added(got_two, g * tp_count, tp_count)).astype(BF16).astype(F32) for g in range(SIDE)]
    )
    scaled = (mixed * gain_b_slab).astype(BF16)
    squares = jnp.broadcast_to(as_line(row_sum(mixed * mixed), 0), (TILE, LANES))
    sz, ff_sems = ff_b[0], fresh_pair()
    for n in range(share):
        for u in range(2):
            product = dot(scaled, gates_b_all[n, u].reshape(slab, LANES))
            for g in range(SIDE):
                tile = product[g * TILE : (g + 1) * TILE]
                if u == 0:
                    tile = jnp.where(sub == GROUP, squares, tile)
                sz[n * SIDE + g, u] = tile.astype(BF16)
        send_pieces(ff_b, ff_sems, n)
    lower = jnp.where(iota((slab, width), 0) == iota((slab, width), 1) + y * width, 1.0, 0.0).astype(BF16)
    residual = dot(mixed.astype(BF16), lower)
    hidden = hidden_units(ff_b, ff_sems)
    send_three, got_three = t_three
    for g in range(SIDE):
        partial = jnp.zeros((ROWS, width), F32)
        for n in range(share):
            partial = partial + dot_rows(hidden[n], down_b_all[n, g])
        send_three[g] = partial.reshape(SIDE, TILE, width).astype(BF16)
    got_three[y * tp_count + tp] = send_three[y]
    three_here = over_plane(lambda far: rows_of(send_three, far), got_three, rows_of)
    with jax.named_scope("plane_three"):
        three_here()
    summed = added(got_three, 0, SIDE * tp_count).reshape(ROWS, width)
    in_use = (iota((ROWS, width), 0) & 7) < GROUP
    last = jnp.where(in_use, residual + 0.5 * summed, 0.0).astype(BF16)

    back = iota((seqs, ROWS), 1)
    seat = lax.shift_right_logical(back, 3) * GROUP + (back & 7)
    lift = jnp.where(((back & 7) < GROUP) & (seat == iota((seqs, ROWS), 0)), 1.0, 0.0).astype(BF16)
    out_tile[...] = dot(lift, last).astype(BF16)
    out_copy = pltpu.make_async_copy(out_tile, out_ref, fresh_sem())
    out_copy.start()

    for condition, ref, sem in sent:
        if condition is None:
            take(ref, sem)
        else:

            @pl.when(condition)
            def _():
                take(ref, sem)

    out_copy.wait()


def on_device(
    ranks,
    tokens,
    gain_first,
    gate_first,
    up_first,
    down_first,
    gain_mixer,
    query_weight,
    key_weight,
    value_weight,
    forget_weight,
    forget_bias,
    key_cache,
    value_cache,
    forget_sum,
    out_weight,
    gain_second,
    gate_second,
    up_second,
    down_second,
):
    kv_count, tp_count = ranks
    depth = kv_count // SIDE
    seqs, length = key_cache.shape[:2]
    chunks = gate_first.shape[1] // LANES
    share = -(-chunks // SIDE)
    pieces = share * SIDE
    width = tokens.shape[1]
    slab = SIDE * width
    dma = pltpu.SemaphoreType.DMA

    def flat(cache):
        return cache.reshape(seqs, 2 * length, LANES)

    operands = [
        tokens,
        gain_first.reshape(1, -1),
        gate_first,
        up_first,
        down_first.T,
        gain_mixer.reshape(1, -1),
        query_weight,
        key_weight,
        value_weight,
        forget_weight.T,
        flat(key_cache),
        flat(value_cache),
        forget_sum,
        out_weight.T,
        gain_second.reshape(1, -1),
        gate_second,
        up_second,
        down_second.T,
    ]

    def half(*dims):
        return pltpu.VMEM(dims, BF16)

    def tiles(*dims):
        return pltpu.VMEM((*dims, TILE, LANES), BF16)

    def ff():
        return (tiles(pieces, 2), tiles(depth, 2), tiles(pieces))

    held = [
        pltpu.VMEM((1, forget_weight.shape[1]), F32),
        half(seqs, width),
        half(1, width),
        half(*gate_first.shape),
        half(*up_first.shape),
        half(1, width),
        half(1, width),
        half(forget_weight.shape[1], slab),
        half(seqs, 2 * length, LANES),
        half(seqs, 2 * length, LANES),
        pltpu.VMEM(forget_sum.shape, F32),
        half(pieces, width, LANES),
        half(pieces, 2, width, LANES),
        half(pieces, width, LANES),
        half(3, SIDE, width, 2 * LANES),
        half(SIDE, width, 2 * LANES),
        half(share, SIDE, width, LANES),
        half(share, 2, SIDE, width, LANES),
        half(share, SIDE, width, LANES),
        dma((17 + 2 * (share + 21),)),
        (pltpu.SemaphoreType.REGULAR, pltpu.SemaphoreType.REGULAR),
        half(seqs, width),
        half(SIDE, TILE, width),
        half(SIDE, TILE, width),
        tiles(SIDE, pieces, 2),
        tiles(SIDE, pieces, 2),
        ff(),
        ff(),
        (
            tiles(depth, 2),
            tiles(depth, 4),
            tiles(SIDE, 2),
            tiles(SIDE, 2),
            tiles(SIDE, 2),
            pltpu.VMEM((SIDE, 1, LANES), F32),
            pltpu.VMEM((SIDE, 1, LANES), F32),
            tiles(depth, 2),
            pltpu.VMEM((depth, 1, LANES), F32),
        ),
        (half(SIDE, TILE, slab), half(SIDE * tp_count, TILE, slab)),
        (half(TILE, slab), half(SIDE * tp_count, TILE, slab)),
        (half(SIDE, SIDE, TILE, width), half(SIDE * tp_count, SIDE, TILE, width)),
        half(SIDE, TILE, slab),
        pltpu.VMEM((SIDE, TILE, 2 * length), F32),
    ]
    return pl.pallas_call(
        functools.partial(layer_kernel, ranks, width * kv_count),
        out_shape=jax.ShapeDtypeStruct(tokens.shape, BF16),
        in_specs=[pl.BlockSpec(memory_space=pltpu.HBM)] * (1 + len(operands)),
        out_specs=pl.BlockSpec(memory_space=pltpu.HBM),
        scratch_shapes=held,
        compiler_params=pltpu.CompilerParams(
            collective_id=0, has_side_effects=True, vmem_limit_bytes=67_043_328
        ),
        name="layer",
    )(forget_bias.reshape(1, -1), *operands)


def solution(mesh):
    ranks = (mesh.shape["kv"], mesh.shape["tp"])
    kv, tp = "kv", "tp"
    in_specs = (
        P(None, kv),
        P(kv),
        P(kv, tp),
        P(kv, tp),
        P(tp, kv),
        P(kv),
        P(kv, tp),
        P(kv, tp),
        P(kv, tp),
        P(),
        P(),
        P(None, kv, tp, None),
        P(None, kv, tp, None),
        P(None, tp, kv),
        P(tp, kv),
        P(kv),
        P(kv, tp),
        P(kv, tp),
        P(tp, kv),
    )
    return jax.shard_map(
        functools.partial(on_device, ranks),
        mesh=mesh,
        in_specs=in_specs,
        out_specs=P(None, kv),
        check_vma=False,
    )
```

```python
import functools

import jax
import jax.numpy as jnp
from jax import lax
from jax.experimental import pallas as pl
from jax.experimental.pallas import tpu as pltpu
from jax.sharding import PartitionSpec as P

MESH = pl.DeviceIdType.MESH
EPSILON = 1e-06
SIDE = 4
GROUP = 6
TILE = 8
ROWS = SIDE * TILE
LANES = 128
F32 = jnp.float32
BF16 = jnp.bfloat16


def dot(left, right):
    return lax.dot_general(left, right, (((1,), (0,)), ((), ())), preferred_element_type=F32)


def dot_rows(left, right):
    return lax.dot_general(left, right, (((1,), (1,)), ((), ())), preferred_element_type=F32)


def iota(shape, dim):
    return lax.broadcasted_iota(jnp.int32, shape, dim)


def far_first(count):
    return sorted(range(1, count), key=lambda k: (-min(k, count - k), k))


def split_value(value, pieces):
    parts = []
    for _ in range(pieces):
        part = value.astype(BF16)
        parts.append(part)
        value = value - part.astype(F32)
    return parts


def layer_kernel(
    ranks,
    features,
    bias_hbm,
    tokens_hbm,
    gain_a_hbm,
    gate_a_hbm,
    up_a_hbm,
    down_a_hbm,
    gain_m_hbm,
    wq_hbm,
    wk_hbm,
    wv_hbm,
    forget_hbm,
    keys_hbm,
    values_hbm,
    decay_hbm,
    wo_hbm,
    gain_b_hbm,
    gate_b_hbm,
    up_b_hbm,
    down_b_hbm,
    out_ref,
    bias,
    tokens,
    gain_a,
    gate_a,
    up_a,
    gain_m,
    gain_b,
    forget,
    keys,
    values,
    decay,
    gates_b,
    down_b,
    w_all,
    wo_all,
    down_a_all,
    gates_b_all,
    down_b_all,
    sems,
    entry_sems,
    out_tile,
    tiles_y,
    tiles_all,
    sy,
    ry,
    ff_a,
    ff_b,
    mix_bufs,
    t_one,
    t_two,
    t_three,
    first_all,
    spread,
):
    kv_count, tp_count = ranks
    depth = kv_count // SIDE
    kv, tp = lax.axis_index("kv"), lax.axis_index("tp")
    z, y = lax.div(kv, SIDE), lax.rem(kv, SIDE)
    chunks = gate_a.shape[1] // LANES
    share = down_b.shape[0] // SIDE
    pieces = share * SIDE
    width = tokens.shape[1]
    slab = SIDE * width
    seqs = tokens.shape[0]
    positions = decay.shape[2]

    def at_z(k):
        return lax.rem(z + k, depth)

    def at_y(k):
        return lax.rem(y + k, SIDE)

    def at_tp(k):
        return lax.rem(tp + k, tp_count)

    z_steps, y_steps = far_first(depth), far_first(SIDE)
    plane = sorted(
        [(a, b) for a in range(SIDE) for b in range(tp_count) if a or b],
        key=lambda s: (-min(s[0], SIDE - s[0]) - min(s[1], tp_count - s[1]) / 2, s),
    )

    counter = iter(range(sems.shape[0]))

    def fresh_sem():
        return sems.at[next(counter)]

    def fresh_pair():
        return fresh_sem(), fresh_sem()

    def take(ref, sem):
        pltpu.make_async_copy(ref, ref, sem).wait()

    barrier = pltpu.get_barrier_semaphore()
    near_sem, far_sem = entry_sems

    def signal(sem, device):
        pl.semaphore_signal(sem, inc=1, device_id=device, device_id_type=MESH)

    for k in z_steps:
        signal(barrier, (at_z(k) * SIDE, tp))
    for k in y_steps:

        @pl.when(at_y(k) != 0)
        def _():
            signal(barrier, (z * SIDE + at_y(k), tp))

    def columns(ref, j):
        return ref.at[:, pl.ds(j * LANES, LANES)]

    loads = {}

    def load(name, whole, *copies):
        sem = fresh_sem()
        for source, target in copies:
            pltpu.make_async_copy(source, target, sem).start()
        loads[name] = (whole, sem)

    def load_one(name, source, target):
        load(name, target, (source, target))

    def loaded(*names):
        for name in names:
            take(*loads.pop(name))

    load_one("tokens", tokens_hbm, tokens)
    load_one("gain_a", gain_a_hbm, gain_a)
    load_one("gate_a", gate_a_hbm, gate_a)
    load_one("up_a", up_a_hbm, up_a)
    load_one("gain_m", gain_m_hbm, gain_m)
    load_one("gain_b", gain_b_hbm, gain_b)
    for k in far_first(tp_count):
        signal(barrier, (z * SIDE, at_tp(k)))
    load_one("down_a", down_a_hbm, down_a_all.at[y])
    load(
        "w",
        w_all.at[:, y],
        (wq_hbm, w_all.at[0, y]),
        (wk_hbm, w_all.at[1, y]),
        (wv_hbm, w_all.at[2, y]),
    )
    load_one("wo", wo_hbm, wo_all.at[y])
    load_one("decay", decay_hbm, decay)
    load_one("bias", bias_hbm, bias)
    load_one("forget", forget_hbm.at[:, pl.ds(pl.multiple_of(z * slab, slab), slab)], forget)
    load_one("keys", keys_hbm, keys)
    load_one("values", values_hbm, values)
    load(
        "gates_b",
        gates_b.at[pl.ds(0, chunks)],
        *[(columns(gate_b_hbm, j), gates_b.at[j, 0]) for j in range(chunks)],
        *[(columns(up_b_hbm, j), gates_b.at[j, 1]) for j in range(chunks)],
    )
    load("down_b", down_b.at[pl.ds(0, chunks)], *[(columns(down_b_hbm, j), down_b.at[j]) for j in range(chunks)])

    sent = []

    def push(source, target, sems, device):
        pltpu.make_async_remote_copy(
            src_ref=source,
            dst_ref=target,
            send_sem=sems[0],
            recv_sem=sems[1],
            device_id=device,
            device_id_type=MESH,
        ).start()

    filled = pl.ds(0, GROUP)

    def rows_of(ref, which):
        return ref.at[which, :, filled]

    def along_y(source_of, target_of, three):
        sems = fresh_pair()
        for k in y_steps:
            far = at_y(k)
            push(source_of(far), target_of(y), sems, (z * SIDE + far, tp))
        sent.append((None, three, sems[0]))
        return lambda: take(three, sems[1])

    def along_z(target, view=lambda ref, which: ref.at[which]):
        sems = fresh_pair()
        for k in z_steps:
            push(view(target, z), view(target, z), sems, (at_z(k) * SIDE + y, tp))
        others = view(target, pl.ds(0, depth - 1))
        sent.append((None, others, sems[0]))
        return lambda: take(others, sems[1])

    def over_plane(source_of, target, view):
        sems = fresh_pair()
        for a, b in plane:
            far = at_y(a)
            push(source_of(far), view(target, y * tp_count + tp), sems, (z * SIDE + far, at_tp(b)))
        others = view(target, pl.ds(0, SIDE * tp_count - 1))
        sent.append((None, others, sems[0]))
        return lambda: take(others, sems[1])

    def over_tp(target):
        sems = fresh_pair()
        for k in far_first(tp_count):
            push(target.at[tp, filled], target.at[tp, filled], sems, (kv, at_tp(k)))
        others = target.at[pl.ds(0, tp_count - 1), filled]
        sent.append((None, others, sems[0]))
        return lambda: take(others, sems[1])

    sub, lane = iota((TILE, LANES), 0), iota((TILE, LANES), 1)

    def column(line, first):
        picked = jnp.where(lane == first + sub, jnp.broadcast_to(line, (TILE, LANES)), 0.0)
        return jnp.sum(picked, axis=1, keepdims=True)

    def as_line(values, first):
        shape = (values.shape[0], LANES)
        spread_out = jnp.where(iota(shape, 1) == first + iota(shape, 0), values, 0.0)
        return jnp.sum(spread_out, axis=0, keepdims=True)

    def row_sum(x):
        return jnp.sum(x, axis=1, keepdims=True)

    def ownership(bufs):
        count = bufs[0].shape[0]

        def piece_of(place):
            return lax.div(count * place + depth - 1, depth)

        def owns(place):
            p = piece_of(place)
            return jnp.logical_and(p < count, lax.div(p * depth, count) == place)

        return count, piece_of, owns

    def send_pieces(bufs, sems, low, high):
        sz, rz, hz = bufs
        _, piece_of, owns = ownership(bufs)
        for k in z_steps:
            far = at_z(k)
            p = piece_of(far)

            @pl.when(owns(far) & (p >= low) & (p < high))
            def _():
                push(sz.at[p], rz.at[z], sems, (far * SIDE + y, tp))

    def hidden_units(bufs, rs_sems, group_of):
        sz, rz, hz = bufs
        pieces, piece_of, owns = ownership(bufs)
        ag_sems = fresh_pair()
        mine_too = jnp.logical_not(owns(z))
        sent.append((owns(z), sz.at[pl.ds(0, pieces - 1)], rs_sems[0]))
        sent.append((mine_too, sz, rs_sems[0]))

        @pl.when(owns(z))
        def _():
            mine = piece_of(z)
            with jax.named_scope("z_reduce"):
                take(rz.at[pl.ds(0, depth - 1)], rs_sems[1])
            rz[z] = sz[mine]
            both = rz[0].astype(F32)
            for k in range(1, depth):
                both = both + rz[k].astype(F32)
            gate_sum, up_sum = both[0], both[1]
            factor = lax.rsqrt(gate_sum[GROUP : GROUP + 1] / features + EPSILON)
            factor = column(factor, group_of(mine) * TILE)
            gate_value, up_value = factor * gate_sum, factor * up_sum
            hidden = gate_value / (1.0 + jnp.exp(-gate_value)) * up_value
            hz[mine] = jnp.where(sub < GROUP, hidden, 0.0).astype(BF16)
            for k in z_steps:
                push(hz.at[mine, filled], hz.at[mine, filled], ag_sems, (at_z(k) * SIDE + y, tp))

        sent.append((owns(z), rz.at[pl.ds(0, depth - 1), 0, filled], ag_sems[0]))
        with jax.named_scope("z_gather"):

            @pl.when(owns(z))
            def _():
                take(hz.at[pl.ds(0, pieces - 1), filled], ag_sems[1])

            @pl.when(mine_too)
            def _():
                take(hz.at[:, filled], ag_sems[1])

    to_rows = iota((ROWS, seqs), 0)
    seat = lax.shift_right_logical(to_rows, 3) * GROUP + (to_rows & 7)
    place = jnp.where(((to_rows & 7) < GROUP) & (seat == iota((ROWS, seqs), 1)), 1.0, 0.0).astype(BF16)

    loaded("tokens", "gain_a", "gain_m", "gain_b")
    x = dot(place, tokens[...])
    gain_rows = [jnp.broadcast_to(g[...].astype(F32), (ROWS, width)) for g in (gain_m, gain_b)]
    row_in_tile = iota((ROWS, width), 0) & 7
    with_gains = jnp.where(row_in_tile == GROUP, gain_rows[0], jnp.where(row_in_tile == GROUP + 1, gain_rows[1], x))
    for g in range(SIDE):
        tiles_y[g] = with_gains[g * TILE : (g + 1) * TILE].astype(BF16)
    tiles_all[y] = tiles_y[y]

    scaled = (x * gain_a[...].astype(F32)).astype(BF16)
    squares = jnp.broadcast_to(as_line(row_sum(x * x), 0), (TILE, LANES))
    loaded("gate_a", "up_a")
    for u, weight in enumerate((gate_a, up_a)):
        product = dot(scaled, weight[...])
        for j in range(chunks):
            for g in range(SIDE):
                tile = product[g * TILE : (g + 1) * TILE, j * LANES : (j + 1) * LANES]
                if u == 0:
                    tile = jnp.where(sub == GROUP, squares, tile)
                sy[g, j, u] = tile.astype(BF16)
    for j in range(chunks, pieces):
        for u in range(2):
            gates_b[j, u] = jnp.zeros((width, LANES), BF16)
        down_b[j] = jnp.zeros((width, LANES), BF16)

    with jax.named_scope("barrier"):

        @pl.when(y != 0)
        def _():
            pl.semaphore_wait(barrier, len(y_steps))
            signal(near_sem, (z * SIDE, tp))

        @pl.when(y == 0)
        def _():
            pl.semaphore_wait(near_sem, len(y_steps))


    portions = [(low, min(low + 4, chunks)) for low in range(0, chunks, 4)]

    def portion(ref, which, n):
        low, high = portions[n]
        return ref.at[which, pl.ds(low, high - low), :, pl.ds(0, GROUP if n else TILE)]

    first_three = pl.ds(0, SIDE - 1)
    reduced = [
        along_y(lambda far: portion(sy, far, n), lambda near: portion(ry, near, n), portion(ry, first_three, n))
        for n in range(len(portions))
    ]
    tiles_here = along_y(lambda far: tiles_y.at[far], lambda near: tiles_all.at[near], tiles_all.at[first_three])
    loaded("down_a")
    down_a_here = along_y(
        lambda far: down_a_all.at[y], lambda near: down_a_all.at[near], down_a_all.at[first_three]
    )
    loaded("w")
    w_here = along_y(lambda far: w_all.at[:, y], lambda near: w_all.at[:, near], w_all.at[:, first_three])
    loaded("wo")
    wo_here = along_y(lambda far: wo_all.at[y], lambda near: wo_all.at[near], wo_all.at[first_three])


    sz, ff_sems = ff_a[0], fresh_pair()
    for n, (low, high) in enumerate(portions):
        with jax.named_scope("y_reduce"):
            reduced[n]()
        rows = pl.ds(low, high - low)
        total = sy[y, rows].astype(F32)
        for k in y_steps:
            total = total + ry[at_y(k), rows].astype(F32)
        if n == 0:
            line = total[0, 0, GROUP : GROUP + 1]
        gates = jnp.where(sub == GROUP, jnp.broadcast_to(line, (TILE, LANES)), total[:, 0])
        sz[rows, 0] = gates.astype(BF16)
        sz[rows, 1] = total[:, 1].astype(BF16)
        if n == 0:
            with jax.named_scope("barrier_far"):

                @pl.when(y == 0)
                def _():
                    pl.semaphore_wait(barrier, SIDE * (len(z_steps) + tp_count - 1))
                    for k in y_steps:
                        signal(far_sem, (z * SIDE + at_y(k), tp))

                @pl.when(y != 0)
                def _():
                    pl.semaphore_wait(far_sem, 1)

        send_pieces(ff_a, ff_sems, low, high)

    loaded("decay")
    woven_all = jnp.zeros((ROWS, 2 * positions), F32)
    thirds = [split_value(decay[:, h, :], 3) for h in range(2)]
    for n in range(3):
        woven = jnp.zeros((seqs, 2 * positions), F32)
        for h in range(2):
            weave = jnp.where(
                iota((positions, 2 * positions), 1) == 2 * iota((positions, 2 * positions), 0) + h, 1.0, 0.0
            ).astype(BF16)
            woven = woven + dot(thirds[h][n], weave)
        woven_all = woven_all + dot(place, woven.astype(BF16))
    for g in range(SIDE):
        spread[g] = woven_all[g * TILE : (g + 1) * TILE]
    tiles_here()
    own_rows = jnp.zeros((TILE, slab), F32)
    for g in range(SIDE):
        lift = jnp.where(iota((width, slab), 1) == iota((width, slab), 0) + g * width, 1.0, 0.0).astype(BF16)
        own_rows = own_rows + dot(tiles_all[g], lift)
    gain_m_slab, gain_b_slab = own_rows[GROUP : GROUP + 1], own_rows[GROUP + 1 : GROUP + 2]
    wide = iota((TILE, slab), 0) < GROUP
    own_rows = jnp.where(wide, own_rows, 0.0)

    hidden_units(ff_a, ff_sems, lambda piece: y)
    hidden = jnp.concatenate([ff_a[2][j] for j in range(chunks)], axis=1)
    with jax.named_scope("down_wait"):
        down_a_here()
    t_one[tp] = dot_rows(hidden, down_a_all[...].reshape(slab, chunks * LANES)).astype(BF16)
    one_here = over_tp(t_one)
    loaded("gates_b")
    with jax.named_scope("plane_one"):
        one_here()

    def added(ref, first, count):
        total = ref[first].astype(F32)
        for k in range(1, count):
            total = total + ref[first + k].astype(F32)
        return total

    summed = added(t_one, 0, tp_count)
    first_rows = (own_rows + 0.5 * summed).astype(BF16)
    first_all[y] = first_rows

    zq, zkv, qf, sa, ra, own_stats, rst, za, zst = mix_bufs
    inverse = LANES ** (-0.5)
    x = first_rows.astype(F32)
    scaled = (x * gain_m_slab).astype(BF16)
    loaded("forget", "bias")
    heads = forget.shape[0]
    r8, c8 = iota((TILE, heads), 0), iota((TILE, heads), 1)
    pick = jnp.where((r8 < 2) & (c8 == 2 * tp + r8), 1.0, 0.0).astype(BF16)
    lines = dot(pick, forget[...])
    biases = row_sum(jnp.where((r8 < 2) & (c8 == 2 * tp + r8), jnp.broadcast_to(bias[...], (TILE, heads)), 0.0))
    side_line = as_line(row_sum(x * x), 0)
    for h in range(2):
        side_line = side_line + as_line(row_sum(scaled.astype(F32) * lines[h : h + 1]), ROWS * (h + 1))
    side_line = jnp.broadcast_to(side_line, (TILE, LANES))
    with jax.named_scope("w_wait"):
        w_here()
    product = [dot(scaled, w_all[u].reshape(slab, 2 * LANES)) for u in range(3)]
    for h in range(2):
        tile = product[0][:, h * LANES : (h + 1) * LANES]
        zq[z, h] = (jnp.where(sub == GROUP, side_line, tile) if h == 0 else tile).astype(BF16)
    zq_here = along_z(zq)
    for u in range(2):
        for h in range(2):
            zkv[z, 2 * u + h] = product[1 + u][:, h * LANES : (h + 1) * LANES].astype(BF16)
    first_here = along_y(
        lambda far: first_all.at[y, filled],
        lambda near: first_all.at[near, filled],
        first_all.at[first_three, filled],
    )
    loaded("down_b")
    down_b_here = along_y(
        lambda far: down_b.at[pl.ds(far * share, share)],
        lambda near: down_b_all.at[:, near],
        down_b_all.at[:, first_three],
    )
    gates_b_all[:, :, y] = gates_b[pl.ds(y * share, share)]
    down_b_all[:, y] = down_b[pl.ds(y * share, share)]

    with jax.named_scope("z_query"):
        zq_here()
    both = zq[0].astype(F32)
    for k in range(1, depth):
        both = both + zq[k].astype(F32)
    line = both[0][GROUP : GROUP + 1]
    factor = column(lax.rsqrt(line / features + EPSILON), 0)
    query = [jnp.where(sub < GROUP, factor * both[h], 0.0).astype(BF16) for h in range(2)]
    for h in range(2):
        qf[y, h] = query[h]
    query_sems = {k: fresh_pair() for k in y_steps}
    for k in y_steps:
        push(rows_of(qf, y), rows_of(qf, y), query_sems[k], (z * SIDE + at_y(k), tp))
        sent.append((None, rows_of(qf, y), query_sems[k][0]))
    zkv_here = along_z(zkv, rows_of)
    log_gate = []
    for h in range(2):
        gate = factor * column(line, ROWS * (h + 1)) + biases[h : h + 1]
        log_gate.append(jnp.minimum(gate, 0.0) - jnp.log(1.0 + jnp.exp(-jnp.abs(gate))))
    loaded("keys", "values")

    lane2, sub2 = iota((TILE, 2 * positions), 1), iota((TILE, 2 * positions), 0)
    even = lax.rem(lane2, 2) == 0
    ra_sems, rst_sems = fresh_pair(), fresh_pair()
    for k in [0, *reversed(y_steps)]:
        g = at_y(k)
        if k:
            with jax.named_scope("y_query"):
                take(rows_of(qf, g), query_sems[SIDE - k][1])
        stats = jnp.zeros((1, LANES), F32)
        pair = jnp.concatenate([jnp.where(sub < GROUP, qf[g, h].astype(F32), 0.0) for h in range(2)]).astype(BF16)
        scores = jnp.zeros((TILE, 2 * positions), F32)
        for i in range(GROUP):
            found = dot_rows(pair, keys[g * GROUP + i])
            found = jnp.where(even, found[:TILE], found[TILE:])
            scores = jnp.where(sub2 == i, found, scores)
        scores = scores * inverse + spread[g]
        tops = [
            jnp.max(jnp.where(even if h == 0 else ~even, scores, -jnp.inf), axis=1, keepdims=True)
            for h in range(2)
        ]
        weights = jnp.exp(scores - jnp.where(even, tops[0], tops[1])).astype(BF16).astype(F32)
        parts = [jnp.where(even, weights, 0.0), jnp.where(even, 0.0, weights)]
        sums = [row_sum(part) for part in parts]
        both_parts = jnp.concatenate(parts).astype(BF16)
        mixed = [jnp.zeros((TILE, LANES), F32) for _ in range(2)]
        for i in range(GROUP):
            found = dot(both_parts, values[g * GROUP + i])
            for h in range(2):
                mixed[h] = jnp.where(sub == i, found[h * TILE : (h + 1) * TILE], mixed[h])
        for h in range(2):
            sa[g, h] = (mixed[h] / sums[h]).astype(BF16)
            stats = stats + as_line(tops[h] + jnp.log(sums[h]), ROWS * h)
        own_stats[g] = stats
        if k:
            push(own_stats.at[g], rst.at[y], rst_sems, (z * SIDE + g, tp))
            push(rows_of(sa, g), rows_of(ra, y), ra_sems, (z * SIDE + g, tp))
    sent.append((None, rows_of(ra, first_three), ra_sems[0]))
    sent.append((None, rst.at[first_three], rst_sems[0]))
    with jax.named_scope("y_merge"):
        take(rst.at[first_three], rst_sems[1])
        take(rows_of(ra, first_three), ra_sems[1])

    def merged(levels, parts):
        top = functools.reduce(jnp.maximum, levels)
        shares = [jnp.exp(level - top) for level in levels]
        whole = sum(shares[1:], shares[0])
        value = sum((a * b for a, b in zip(shares[1:], parts[1:])), shares[0] * parts[0])
        return value / whole, top + jnp.log(whole)

    spots = [y] + [at_y(k) for k in y_steps]
    stats = jnp.zeros((1, LANES), F32)
    for h in range(2):
        levels = [column(own_stats[y], ROWS * h)] + [column(rst[spot], ROWS * h) for spot in spots[1:]]
        parts = [sa[y, h].astype(F32)] + [ra[spot, h].astype(F32) for spot in spots[1:]]
        value, level = merged(levels, parts)
        za[z, h] = value.astype(BF16)
        stats = stats + as_line(level, ROWS * h)
    zst[z] = stats
    zst_here = along_z(zst)
    za_here = along_z(za, rows_of)

    gates_b_here = along_y(
        lambda far: gates_b.at[pl.ds(far * share, share)],
        lambda near: gates_b_all.at[:, :, near],
        gates_b_all.at[:, :, first_three],
    )

    with jax.named_scope("z_keyvalue"):
        zkv_here()
    both = zkv[0].astype(F32)
    for k in range(1, depth):
        both = both + zkv[k].astype(F32)
    fresh = [jnp.where(sub < GROUP, factor * both[u], 0.0).astype(BF16).astype(F32) for u in range(4)]
    own_level = [row_sum(query[h].astype(F32) * fresh[h]) * inverse for h in range(2)]
    first_here()
    gates_b_here()
    down_b_here()
    wo_here()
    with jax.named_scope("z_merge"):
        zst_here()
        za_here()
    attended = []
    for h in range(2):
        levels = [column(zst[k], ROWS * h) + log_gate[h] for k in range(depth)] + [own_level[h]]
        parts = [za[k, h].astype(F32) for k in range(depth)] + [fresh[2 + h]]
        attended.append(merged(levels, parts)[0])
    attended = jnp.concatenate(attended, axis=1).astype(BF16)
    send_two, got_two = t_two
    mine = dot_rows(attended, wo_all[...].reshape(slab, 2 * LANES)).astype(BF16)
    send_two[...] = mine
    got_two[y * tp_count + tp] = mine
    two_here = over_plane(lambda far: send_two.at[filled], got_two, lambda ref, which: ref.at[which, filled])
    with jax.named_scope("plane_two"):
        two_here()

    mixed = jnp.concatenate(
        [(first_all[g].astype(F32) + added(got_two, g * tp_count, tp_count)).astype(BF16).astype(F32) for g in range(SIDE)]
    )
    scaled = (mixed * gain_b_slab).astype(BF16)
    squares = jnp.broadcast_to(as_line(row_sum(mixed * mixed), 0), (TILE, LANES))
    sz, ff_sems = ff_b[0], fresh_pair()
    for n in range(share):
        for u in range(2):
            product = dot(scaled, gates_b_all[n, u].reshape(slab, LANES))
            for g in range(SIDE):
                tile = product[g * TILE : (g + 1) * TILE]
                if u == 0:
                    tile = jnp.where(sub == GROUP, squares, tile)
                sz[n * SIDE + g, u] = tile.astype(BF16)
        send_pieces(ff_b, ff_sems, n * SIDE, (n + 1) * SIDE)
    lower = jnp.where(iota((slab, width), 0) == iota((slab, width), 1) + y * width, 1.0, 0.0).astype(BF16)
    residual = dot(mixed.astype(BF16), lower)
    hidden_units(ff_b, ff_sems, lambda piece: lax.rem(piece, SIDE))
    hidden = [
        ff_b[2][n * SIDE : (n + 1) * SIDE].astype(F32).reshape(ROWS, LANES).astype(BF16) for n in range(share)
    ]
    send_three, got_three = t_three
    for g in range(SIDE):
        partial = jnp.zeros((ROWS, width), F32)
        for n in range(share):
            partial = partial + dot_rows(hidden[n], down_b_all[n, g])
        send_three[g] = partial.reshape(SIDE, TILE, width).astype(BF16)
    got_three[y * tp_count + tp] = send_three[y]
    three_here = over_plane(lambda far: rows_of(send_three, far), got_three, rows_of)
    with jax.named_scope("plane_three"):
        three_here()
    summed = added(got_three, 0, SIDE * tp_count).reshape(ROWS, width)
    in_use = (iota((ROWS, width), 0) & 7) < GROUP
    last = jnp.where(in_use, residual + 0.5 * summed, 0.0).astype(BF16)

    back = iota((seqs, ROWS), 1)
    seat = lax.shift_right_logical(back, 3) * GROUP + (back & 7)
    lift = jnp.where(((back & 7) < GROUP) & (seat == iota((seqs, ROWS), 0)), 1.0, 0.0).astype(BF16)
    out_tile[...] = dot(lift, last).astype(BF16)
    out_copy = pltpu.make_async_copy(out_tile, out_ref, fresh_sem())
    out_copy.start()

    for condition, ref, sem in sent:
        if condition is None:
            take(ref, sem)
        else:

            @pl.when(condition)
            def _():
                take(ref, sem)

    out_copy.wait()


def on_device(
    ranks,
    tokens,
    gain_first,
    gate_first,
    up_first,
    down_first,
    gain_mixer,
    query_weight,
    key_weight,
    value_weight,
    forget_weight,
    forget_bias,
    key_cache,
    value_cache,
    forget_sum,
    out_weight,
    gain_second,
    gate_second,
    up_second,
    down_second,
):
    kv_count, tp_count = ranks
    depth = kv_count // SIDE
    seqs, length = key_cache.shape[:2]
    chunks = gate_first.shape[1] // LANES
    share = -(-chunks // SIDE)
    pieces = share * SIDE
    width = tokens.shape[1]
    slab = SIDE * width
    dma = pltpu.SemaphoreType.DMA

    def flat(cache):
        return cache.reshape(seqs, 2 * length, LANES)

    operands = [
        tokens,
        gain_first.reshape(1, -1),
        gate_first,
        up_first,
        down_first.T,
        gain_mixer.reshape(1, -1),
        query_weight,
        key_weight,
        value_weight,
        forget_weight.T,
        flat(key_cache),
        flat(value_cache),
        forget_sum,
        out_weight.T,
        gain_second.reshape(1, -1),
        gate_second,
        up_second,
        down_second.T,
    ]

    def half(*dims):
        return pltpu.VMEM(dims, BF16)

    def tiles(*dims):
        return pltpu.VMEM((*dims, TILE, LANES), BF16)

    def ff(count):
        return (tiles(count, 2), tiles(depth, 2), tiles(count))

    held = [
        pltpu.VMEM((1, forget_weight.shape[1]), F32),
        half(seqs, width),
        half(1, width),
        half(*gate_first.shape),
        half(*up_first.shape),
        half(1, width),
        half(1, width),
        half(forget_weight.shape[1], slab),
        half(seqs, 2 * length, LANES),
        half(seqs, 2 * length, LANES),
        pltpu.VMEM(forget_sum.shape, F32),
        half(pieces, 2, width, LANES),
        half(pieces, width, LANES),
        half(3, SIDE, width, 2 * LANES),
        half(SIDE, width, 2 * LANES),
        half(SIDE, width, chunks * LANES),
        half(share, 2, SIDE, width, LANES),
        half(share, SIDE, width, LANES),
        dma((17 + 2 * (-(-chunks // 4) + 23),)),
        (pltpu.SemaphoreType.REGULAR, pltpu.SemaphoreType.REGULAR),
        half(seqs, width),
        half(SIDE, TILE, width),
        half(SIDE, TILE, width),
        tiles(SIDE, chunks, 2),
        tiles(SIDE, chunks, 2),
        ff(chunks),
        ff(pieces),
        (
            tiles(depth, 2),
            tiles(depth, 4),
            tiles(SIDE, 2),
            tiles(SIDE, 2),
            tiles(SIDE, 2),
            pltpu.VMEM((SIDE, 1, LANES), F32),
            pltpu.VMEM((SIDE, 1, LANES), F32),
            tiles(depth, 2),
            pltpu.VMEM((depth, 1, LANES), F32),
        ),
        half(tp_count, TILE, slab),
        (half(TILE, slab), half(SIDE * tp_count, TILE, slab)),
        (half(SIDE, SIDE, TILE, width), half(SIDE * tp_count, SIDE, TILE, width)),
        half(SIDE, TILE, slab),
        pltpu.VMEM((SIDE, TILE, 2 * length), F32),
    ]
    return pl.pallas_call(
        functools.partial(layer_kernel, ranks, width * kv_count),
        out_shape=jax.ShapeDtypeStruct(tokens.shape, BF16),
        in_specs=[pl.BlockSpec(memory_space=pltpu.HBM)] * (1 + len(operands)),
        out_specs=pl.BlockSpec(memory_space=pltpu.HBM),
        scratch_shapes=held,
        compiler_params=pltpu.CompilerParams(
            collective_id=0, has_side_effects=True, vmem_limit_bytes=67_043_328
        ),
        name="layer",
    )(forget_bias.reshape(1, -1), *operands)


def solution(mesh):
    ranks = (mesh.shape["kv"], mesh.shape["tp"])
    kv, tp = "kv", "tp"
    in_specs = (
        P(None, kv),
        P(kv),
        P(kv, tp),
        P(kv, tp),
        P(tp, kv),
        P(kv),
        P(kv, tp),
        P(kv, tp),
        P(kv, tp),
        P(),
        P(),
        P(None, kv, tp, None),
        P(None, kv, tp, None),
        P(None, tp, kv),
        P(tp, kv),
        P(kv),
        P(kv, tp),
        P(kv, tp),
        P(tp, kv),
    )
    return jax.shard_map(
        functools.partial(on_device, ranks),
        mesh=mesh,
        in_specs=in_specs,
        out_specs=P(None, kv),
        check_vma=False,
    )
```

```python
import functools

import jax
import jax.numpy as jnp
from jax import lax
from jax.experimental import pallas as pl
from jax.experimental.pallas import tpu as pltpu
from jax.sharding import PartitionSpec as P

MESH = pl.DeviceIdType.MESH
EPSILON = 1e-06
SIDE = 4
GROUP = 6
TILE = 8
ROWS = SIDE * TILE
LANES = 128
F32 = jnp.float32
BF16 = jnp.bfloat16


def dot(left, right):
    return lax.dot_general(left, right, (((1,), (0,)), ((), ())), preferred_element_type=F32)


def dot_rows(left, right):
    return lax.dot_general(left, right, (((1,), (1,)), ((), ())), preferred_element_type=F32)


def iota(shape, dim):
    return lax.broadcasted_iota(jnp.int32, shape, dim)


def far_first(count):
    return sorted(range(1, count), key=lambda k: (-min(k, count - k), k))


def split_value(value, pieces):
    parts = []
    for _ in range(pieces):
        part = value.astype(BF16)
        parts.append(part)
        value = value - part.astype(F32)
    return parts


def layer_kernel(
    ranks,
    features,
    bias_hbm,
    tokens_hbm,
    gain_a_hbm,
    gate_a_hbm,
    up_a_hbm,
    down_a_hbm,
    gain_m_hbm,
    wq_hbm,
    wk_hbm,
    wv_hbm,
    forget_hbm,
    keys_hbm,
    values_hbm,
    decay_hbm,
    wo_hbm,
    gain_b_hbm,
    gate_b_hbm,
    up_b_hbm,
    down_b_hbm,
    out_ref,
    bias,
    tokens,
    gain_a,
    gate_a,
    up_a,
    gain_m,
    gain_b,
    forget,
    keys,
    values,
    decay,
    gates_b,
    down_b,
    w_all,
    wo_all,
    down_a_all,
    gates_b_all,
    down_b_all,
    sems,
    entry_sems,
    out_tile,
    tiles_y,
    tiles_all,
    sy,
    ry,
    ff_a,
    ff_b,
    mix_bufs,
    t_one,
    t_two,
    t_three,
    first_all,
    spread,
):
    kv_count, tp_count = ranks
    depth = kv_count // SIDE
    kv, tp = lax.axis_index("kv"), lax.axis_index("tp")
    z, y = lax.div(kv, SIDE), lax.rem(kv, SIDE)
    chunks = gate_a.shape[1] // LANES
    share = down_b.shape[0] // SIDE
    pieces = share * SIDE
    width = tokens.shape[1]
    slab = SIDE * width
    seqs = tokens.shape[0]
    positions = decay.shape[2]

    def at_z(k):
        return lax.rem(z + k, depth)

    def at_y(k):
        return lax.rem(y + k, SIDE)

    def at_tp(k):
        return lax.rem(tp + k, tp_count)

    z_steps, y_steps = far_first(depth), far_first(SIDE)
    plane = sorted(
        [(a, b) for a in range(SIDE) for b in range(tp_count) if a or b],
        key=lambda s: (-min(s[0], SIDE - s[0]) - min(s[1], tp_count - s[1]) / 2, s),
    )

    counter = iter(range(sems.shape[0]))

    def fresh_sem():
        return sems.at[next(counter)]

    def fresh_pair():
        return fresh_sem(), fresh_sem()

    def take(ref, sem):
        pltpu.make_async_copy(ref, ref, sem).wait()

    barrier = pltpu.get_barrier_semaphore()
    near_sem, far_sem = entry_sems

    def signal(sem, device):
        pl.semaphore_signal(sem, inc=1, device_id=device, device_id_type=MESH)

    for k in z_steps:
        signal(barrier, (at_z(k) * SIDE, tp))
    for k in y_steps:

        @pl.when(at_y(k) != 0)
        def _():
            signal(barrier, (z * SIDE + at_y(k), tp))

    def columns(ref, j):
        return ref.at[:, pl.ds(j * LANES, LANES)]

    loads = {}

    def load(name, whole, *copies):
        sem = fresh_sem()
        for source, target in copies:
            pltpu.make_async_copy(source, target, sem).start()
        loads[name] = (whole, sem)

    def load_one(name, source, target):
        load(name, target, (source, target))

    def loaded(*names):
        for name in names:
            take(*loads.pop(name))

    load_one("tokens", tokens_hbm, tokens)
    load_one("gain_a", gain_a_hbm, gain_a)
    load_one("gate_a", gate_a_hbm, gate_a)
    load_one("up_a", up_a_hbm, up_a)
    load_one("gain_m", gain_m_hbm, gain_m)
    load_one("gain_b", gain_b_hbm, gain_b)
    for k in far_first(tp_count):
        signal(barrier, (z * SIDE, at_tp(k)))
    load_one("down_a", down_a_hbm, down_a_all.at[y])
    load(
        "w",
        w_all.at[:, y],
        (wq_hbm, w_all.at[0, y]),
        (wk_hbm, w_all.at[1, y]),
        (wv_hbm, w_all.at[2, y]),
    )
    load_one("wo", wo_hbm, wo_all.at[y])
    load_one("decay", decay_hbm, decay)
    load_one("bias", bias_hbm, bias)
    load_one("forget", forget_hbm.at[:, pl.ds(pl.multiple_of(z * slab, slab), slab)], forget)
    load_one("keys", keys_hbm, keys)
    load_one("values", values_hbm, values)
    load(
        "gates_b",
        gates_b.at[pl.ds(0, chunks)],
        *[(columns(gate_b_hbm, j), gates_b.at[j, 0]) for j in range(chunks)],
        *[(columns(up_b_hbm, j), gates_b.at[j, 1]) for j in range(chunks)],
    )
    load("down_b", down_b.at[pl.ds(0, chunks)], *[(columns(down_b_hbm, j), down_b.at[j]) for j in range(chunks)])

    sent = []

    def push(source, target, sems, device):
        pltpu.make_async_remote_copy(
            src_ref=source,
            dst_ref=target,
            send_sem=sems[0],
            recv_sem=sems[1],
            device_id=device,
            device_id_type=MESH,
        ).start()

    filled = pl.ds(0, GROUP)

    def rows_of(ref, which):
        return ref.at[which, :, filled]

    def along_y(source_of, target_of, three):
        sems = fresh_pair()
        for k in y_steps:
            far = at_y(k)
            push(source_of(far), target_of(y), sems, (z * SIDE + far, tp))
        sent.append((None, three, sems[0]))
        return lambda: take(three, sems[1])

    def whole_of(ref, which):
        return ref.at[which]

    def along_z_together(*targets):
        pairs = [fresh_pair() for _ in targets]
        for k in z_steps:
            for (target, view), sems in zip(targets, pairs):
                push(view(target, z), view(target, z), sems, (at_z(k) * SIDE + y, tp))
        arrivals = []
        for (target, view), sems in zip(targets, pairs):
            others = view(target, pl.ds(0, depth - 1))
            sent.append((None, others, sems[0]))
            arrivals.append(functools.partial(take, others, sems[1]))
        return arrivals

    def along_z(target, view=whole_of):
        return along_z_together((target, view))[0]

    def over_plane(source_of, target, view):
        sems = fresh_pair()
        for a, b in plane:
            far = at_y(a)
            push(source_of(far), view(target, y * tp_count + tp), sems, (z * SIDE + far, at_tp(b)))
        others = view(target, pl.ds(0, SIDE * tp_count - 1))
        sent.append((None, others, sems[0]))
        return lambda: take(others, sems[1])

    def over_tp(target):
        sems = fresh_pair()
        for k in far_first(tp_count):
            push(target.at[tp, filled], target.at[tp, filled], sems, (kv, at_tp(k)))
        others = target.at[pl.ds(0, tp_count - 1), filled]
        sent.append((None, others, sems[0]))
        return lambda: take(others, sems[1])

    sub, lane = iota((TILE, LANES), 0), iota((TILE, LANES), 1)

    def column(line, first):
        picked = jnp.where(lane == first + sub, jnp.broadcast_to(line, (TILE, LANES)), 0.0)
        return jnp.sum(picked, axis=1, keepdims=True)

    def as_line(values, first):
        shape = (values.shape[0], LANES)
        spread_out = jnp.where(iota(shape, 1) == first + iota(shape, 0), values, 0.0)
        return jnp.sum(spread_out, axis=0, keepdims=True)

    def row_sum(x):
        return jnp.sum(x, axis=1, keepdims=True)

    def ownership(bufs):
        count = bufs[0].shape[0]

        def piece_of(place):
            return lax.div(count * place + depth - 1, depth)

        def owns(place):
            p = piece_of(place)
            return jnp.logical_and(p < count, lax.div(p * depth, count) == place)

        return count, piece_of, owns

    def send_pieces(bufs, sems, low, high):
        sz, rz, hz = bufs
        _, piece_of, owns = ownership(bufs)
        for k in z_steps:
            far = at_z(k)
            p = piece_of(far)

            @pl.when(owns(far) & (p >= low) & (p < high))
            def _():
                push(sz.at[p], rz.at[z], sems, (far * SIDE + y, tp))

    def hidden_units(bufs, rs_sems, group_of):
        sz, rz, hz = bufs
        pieces, piece_of, owns = ownership(bufs)
        ag_sems = fresh_pair()
        mine_too = jnp.logical_not(owns(z))
        sent.append((owns(z), sz.at[pl.ds(0, pieces - 1)], rs_sems[0]))
        sent.append((mine_too, sz, rs_sems[0]))

        @pl.when(owns(z))
        def _():
            mine = piece_of(z)
            with jax.named_scope("z_reduce"):
                take(rz.at[pl.ds(0, depth - 1)], rs_sems[1])
            rz[z] = sz[mine]
            both = rz[0].astype(F32)
            for k in range(1, depth):
                both = both + rz[k].astype(F32)
            gate_sum, up_sum = both[0], both[1]
            factor = lax.rsqrt(gate_sum[GROUP : GROUP + 1] / features + EPSILON)
            factor = column(factor, group_of(mine) * TILE)
            gate_value, up_value = factor * gate_sum, factor * up_sum
            hidden = gate_value / (1.0 + jnp.exp(-gate_value)) * up_value
            hz[mine] = jnp.where(sub < GROUP, hidden, 0.0).astype(BF16)
            for k in z_steps:
                push(hz.at[mine, filled], hz.at[mine, filled], ag_sems, (at_z(k) * SIDE + y, tp))

        sent.append((owns(z), rz.at[pl.ds(0, depth - 1), 0, filled], ag_sems[0]))
        with jax.named_scope("z_gather"):

            @pl.when(owns(z))
            def _():
                take(hz.at[pl.ds(0, pieces - 1), filled], ag_sems[1])

            @pl.when(mine_too)
            def _():
                take(hz.at[:, filled], ag_sems[1])

    to_rows = iota((ROWS, seqs), 0)
    seat = lax.shift_right_logical(to_rows, 3) * GROUP + (to_rows & 7)
    place = jnp.where(((to_rows & 7) < GROUP) & (seat == iota((ROWS, seqs), 1)), 1.0, 0.0).astype(BF16)

    loaded("tokens", "gain_a", "gain_m", "gain_b")
    x = dot(place, tokens[...])
    gain_rows = [jnp.broadcast_to(g[...].astype(F32), (ROWS, width)) for g in (gain_m, gain_b)]
    row_in_tile = iota((ROWS, width), 0) & 7
    with_gains = jnp.where(row_in_tile == GROUP, gain_rows[0], jnp.where(row_in_tile == GROUP + 1, gain_rows[1], x))
    for g in range(SIDE):
        tiles_y[g] = with_gains[g * TILE : (g + 1) * TILE].astype(BF16)
    tiles_all[y] = tiles_y[y]

    scaled = (x * gain_a[...].astype(F32)).astype(BF16)
    squares = jnp.broadcast_to(as_line(row_sum(x * x), 0), (TILE, LANES))
    loaded("gate_a", "up_a")
    for u, weight in enumerate((gate_a, up_a)):
        product = dot(scaled, weight[...])
        for j in range(chunks):
            for g in range(SIDE):
                tile = product[g * TILE : (g + 1) * TILE, j * LANES : (j + 1) * LANES]
                if u == 0:
                    tile = jnp.where(sub == GROUP, squares, tile)
                sy[g, j, u] = tile.astype(BF16)
    for j in range(chunks, pieces):
        for u in range(2):
            gates_b[j, u] = jnp.zeros((width, LANES), BF16)
        down_b[j] = jnp.zeros((width, LANES), BF16)

    with jax.named_scope("barrier"):

        @pl.when(y != 0)
        def _():
            pl.semaphore_wait(barrier, len(y_steps))
            signal(near_sem, (z * SIDE, tp))

        @pl.when(y == 0)
        def _():
            pl.semaphore_wait(near_sem, len(y_steps))


    portions = [(low, min(low + 4, chunks)) for low in range(0, chunks, 4)]

    def portion(ref, which, n):
        low, high = portions[n]
        return ref.at[which, pl.ds(low, high - low), :, pl.ds(0, GROUP if n else TILE)]

    first_three = pl.ds(0, SIDE - 1)
    reduced = [
        along_y(lambda far: portion(sy, far, n), lambda near: portion(ry, near, n), portion(ry, first_three, n))
        for n in range(len(portions))
    ]
    tiles_here = along_y(lambda far: tiles_y.at[far], lambda near: tiles_all.at[near], tiles_all.at[first_three])
    loaded("down_a")
    down_a_here = along_y(
        lambda far: down_a_all.at[y], lambda near: down_a_all.at[near], down_a_all.at[first_three]
    )
    loaded("w")
    w_here = along_y(lambda far: w_all.at[:, y], lambda near: w_all.at[:, near], w_all.at[:, first_three])
    loaded("wo")
    wo_here = along_y(lambda far: wo_all.at[y], lambda near: wo_all.at[near], wo_all.at[first_three])


    sz, ff_sems = ff_a[0], fresh_pair()
    for n, (low, high) in enumerate(portions):
        with jax.named_scope("y_reduce"):
            reduced[n]()
        rows = pl.ds(low, high - low)
        total = sy[y, rows].astype(F32)
        for k in y_steps:
            total = total + ry[at_y(k), rows].astype(F32)
        if n == 0:
            line = total[0, 0, GROUP : GROUP + 1]
        gates = jnp.where(sub == GROUP, jnp.broadcast_to(line, (TILE, LANES)), total[:, 0])
        sz[rows, 0] = gates.astype(BF16)
        sz[rows, 1] = total[:, 1].astype(BF16)
        if n == 0:
            with jax.named_scope("barrier_far"):

                @pl.when(y == 0)
                def _():
                    pl.semaphore_wait(barrier, SIDE * (len(z_steps) + tp_count - 1))
                    for k in y_steps:
                        signal(far_sem, (z * SIDE + at_y(k), tp))

                @pl.when(y != 0)
                def _():
                    pl.semaphore_wait(far_sem, 1)

        send_pieces(ff_a, ff_sems, low, high)

    loaded("decay")
    woven_all = jnp.zeros((ROWS, 2 * positions), F32)
    thirds = [split_value(decay[:, h, :], 3) for h in range(2)]
    for n in range(3):
        woven = jnp.zeros((seqs, 2 * positions), F32)
        for h in range(2):
            weave = jnp.where(
                iota((positions, 2 * positions), 1) == 2 * iota((positions, 2 * positions), 0) + h, 1.0, 0.0
            ).astype(BF16)
            woven = woven + dot(thirds[h][n], weave)
        woven_all = woven_all + dot(place, woven.astype(BF16))
    for g in range(SIDE):
        spread[g] = woven_all[g * TILE : (g + 1) * TILE]
    tiles_here()
    own_rows = jnp.zeros((TILE, slab), F32)
    for g in range(SIDE):
        lift = jnp.where(iota((width, slab), 1) == iota((width, slab), 0) + g * width, 1.0, 0.0).astype(BF16)
        own_rows = own_rows + dot(tiles_all[g], lift)
    gain_m_slab, gain_b_slab = own_rows[GROUP : GROUP + 1], own_rows[GROUP + 1 : GROUP + 2]
    wide = iota((TILE, slab), 0) < GROUP
    own_rows = jnp.where(wide, own_rows, 0.0)

    hidden_units(ff_a, ff_sems, lambda piece: y)
    hidden = jnp.concatenate([ff_a[2][j] for j in range(chunks)], axis=1)
    with jax.named_scope("down_wait"):
        down_a_here()
    t_one[tp] = dot_rows(hidden, down_a_all[...].reshape(slab, chunks * LANES)).astype(BF16)
    one_here = over_tp(t_one)
    loaded("gates_b")
    with jax.named_scope("plane_one"):
        one_here()

    def added(ref, first, count):
        total = ref[first].astype(F32)
        for k in range(1, count):
            total = total + ref[first + k].astype(F32)
        return total

    summed = added(t_one, 0, tp_count)
    first_rows = (own_rows + 0.5 * summed).astype(BF16)
    first_all[y] = first_rows

    zq, zkv, qf, sa, ra, own_stats, rst, za, zst = mix_bufs
    inverse = LANES ** (-0.5)
    x = first_rows.astype(F32)
    scaled = (x * gain_m_slab).astype(BF16)
    loaded("forget", "bias")
    heads = forget.shape[0]
    r8, c8 = iota((TILE, heads), 0), iota((TILE, heads), 1)
    pick = jnp.where((r8 < 2) & (c8 == 2 * tp + r8), 1.0, 0.0).astype(BF16)
    lines = dot(pick, forget[...])
    biases = row_sum(jnp.where((r8 < 2) & (c8 == 2 * tp + r8), jnp.broadcast_to(bias[...], (TILE, heads)), 0.0))
    side_line = as_line(row_sum(x * x), 0)
    for h in range(2):
        side_line = side_line + as_line(row_sum(scaled.astype(F32) * lines[h : h + 1]), ROWS * (h + 1))
    side_line = jnp.broadcast_to(side_line, (TILE, LANES))
    with jax.named_scope("w_wait"):
        w_here()
    product = [dot(scaled, w_all[u].reshape(slab, 2 * LANES)) for u in range(3)]
    for h in range(2):
        tile = product[0][:, h * LANES : (h + 1) * LANES]
        zq[z, h] = (jnp.where(sub == GROUP, side_line, tile) if h == 0 else tile).astype(BF16)
    zq_here = along_z(zq)
    for u in range(2):
        for h in range(2):
            zkv[z, 2 * u + h] = product[1 + u][:, h * LANES : (h + 1) * LANES].astype(BF16)
    first_here = along_y(
        lambda far: first_all.at[y, filled],
        lambda near: first_all.at[near, filled],
        first_all.at[first_three, filled],
    )
    loaded("down_b")
    down_b_here = along_y(
        lambda far: down_b.at[pl.ds(far * share, share)],
        lambda near: down_b_all.at[:, near],
        down_b_all.at[:, first_three],
    )
    gates_b_all[:, :, y] = gates_b[pl.ds(y * share, share)]
    down_b_all[:, y] = down_b[pl.ds(y * share, share)]

    with jax.named_scope("z_query"):
        zq_here()
    both = zq[0].astype(F32)
    for k in range(1, depth):
        both = both + zq[k].astype(F32)
    line = both[0][GROUP : GROUP + 1]
    factor = column(lax.rsqrt(line / features + EPSILON), 0)
    query = [jnp.where(sub < GROUP, factor * both[h], 0.0).astype(BF16) for h in range(2)]
    for h in range(2):
        qf[y, h] = query[h]
    query_sems = {k: fresh_pair() for k in y_steps}
    for k in y_steps:
        push(rows_of(qf, y), rows_of(qf, y), query_sems[k], (z * SIDE + at_y(k), tp))
        sent.append((None, rows_of(qf, y), query_sems[k][0]))
    zkv_here = along_z(zkv, rows_of)
    log_gate = []
    for h in range(2):
        gate = factor * column(line, ROWS * (h + 1)) + biases[h : h + 1]
        log_gate.append(jnp.minimum(gate, 0.0) - jnp.log(1.0 + jnp.exp(-jnp.abs(gate))))
    loaded("keys", "values")

    lane2, sub2 = iota((TILE, 2 * positions), 1), iota((TILE, 2 * positions), 0)
    even = lax.rem(lane2, 2) == 0
    ra_sems, rst_sems = fresh_pair(), fresh_pair()
    for k in [0, *reversed(y_steps)]:
        g = at_y(k)
        if k:
            with jax.named_scope("y_query"):
                take(rows_of(qf, g), query_sems[SIDE - k][1])
        stats = jnp.zeros((1, LANES), F32)
        pair = jnp.concatenate([jnp.where(sub < GROUP, qf[g, h].astype(F32), 0.0) for h in range(2)]).astype(BF16)
        scores = jnp.zeros((TILE, 2 * positions), F32)
        for i in range(GROUP):
            found = dot_rows(pair, keys[g * GROUP + i])
            found = jnp.where(even, found[:TILE], found[TILE:])
            scores = jnp.where(sub2 == i, found, scores)
        scores = scores * inverse + spread[g]
        tops = [
            jnp.max(jnp.where(even if h == 0 else ~even, scores, -jnp.inf), axis=1, keepdims=True)
            for h in range(2)
        ]
        weights = jnp.exp(scores - jnp.where(even, tops[0], tops[1])).astype(BF16).astype(F32)
        parts = [jnp.where(even, weights, 0.0), jnp.where(even, 0.0, weights)]
        sums = [row_sum(part) for part in parts]
        both_parts = jnp.concatenate(parts).astype(BF16)
        mixed = [jnp.zeros((TILE, LANES), F32) for _ in range(2)]
        for i in range(GROUP):
            found = dot(both_parts, values[g * GROUP + i])
            for h in range(2):
                mixed[h] = jnp.where(sub == i, found[h * TILE : (h + 1) * TILE], mixed[h])
        for h in range(2):
            sa[g, h] = (mixed[h] / sums[h]).astype(BF16)
            stats = stats + as_line(tops[h] + jnp.log(sums[h]), ROWS * h)
        own_stats[g] = stats
        if k:
            push(own_stats.at[g], rst.at[y], rst_sems, (z * SIDE + g, tp))
            push(rows_of(sa, g), rows_of(ra, y), ra_sems, (z * SIDE + g, tp))
    sent.append((None, rows_of(ra, first_three), ra_sems[0]))
    sent.append((None, rst.at[first_three], rst_sems[0]))
    with jax.named_scope("y_merge"):
        take(rst.at[first_three], rst_sems[1])
        take(rows_of(ra, first_three), ra_sems[1])

    def merged(levels, parts):
        top = functools.reduce(jnp.maximum, levels)
        shares = [jnp.exp(level - top) for level in levels]
        whole = sum(shares[1:], shares[0])
        value = sum((a * b for a, b in zip(shares[1:], parts[1:])), shares[0] * parts[0])
        return value / whole, top + jnp.log(whole)

    spots = [y] + [at_y(k) for k in y_steps]
    stats = jnp.zeros((1, LANES), F32)
    for h in range(2):
        levels = [column(own_stats[y], ROWS * h)] + [column(rst[spot], ROWS * h) for spot in spots[1:]]
        parts = [sa[y, h].astype(F32)] + [ra[spot, h].astype(F32) for spot in spots[1:]]
        value, level = merged(levels, parts)
        za[z, h] = value.astype(BF16)
        stats = stats + as_line(level, ROWS * h)
    zst[z] = stats
    za_here, zst_here = along_z_together((za, rows_of), (zst, whole_of))

    gates_b_here = along_y(
        lambda far: gates_b.at[pl.ds(far * share, share)],
        lambda near: gates_b_all.at[:, :, near],
        gates_b_all.at[:, :, first_three],
    )

    with jax.named_scope("z_keyvalue"):
        zkv_here()
    both = zkv[0].astype(F32)
    for k in range(1, depth):
        both = both + zkv[k].astype(F32)
    fresh = [jnp.where(sub < GROUP, factor * both[u], 0.0).astype(BF16).astype(F32) for u in range(4)]
    own_level = [row_sum(query[h].astype(F32) * fresh[h]) * inverse for h in range(2)]
    first_here()
    gates_b_here()
    down_b_here()
    wo_here()
    with jax.named_scope("z_merge"):
        zst_here()
        za_here()
    attended = []
    for h in range(2):
        levels = [column(zst[k], ROWS * h) + log_gate[h] for k in range(depth)] + [own_level[h]]
        parts = [za[k, h].astype(F32) for k in range(depth)] + [fresh[2 + h]]
        attended.append(merged(levels, parts)[0])
    attended = jnp.concatenate(attended, axis=1).astype(BF16)
    send_two, got_two = t_two
    mine = dot_rows(attended, wo_all[...].reshape(slab, 2 * LANES)).astype(BF16)
    send_two[...] = mine
    got_two[y * tp_count + tp] = mine
    two_here = over_plane(lambda far: send_two.at[filled], got_two, lambda ref, which: ref.at[which, filled])
    with jax.named_scope("plane_two"):
        two_here()

    mixed = jnp.concatenate(
        [(first_all[g].astype(F32) + added(got_two, g * tp_count, tp_count)).astype(BF16).astype(F32) for g in range(SIDE)]
    )
    scaled = (mixed * gain_b_slab).astype(BF16)
    squares = jnp.broadcast_to(as_line(row_sum(mixed * mixed), 0), (TILE, LANES))
    sz, ff_sems = ff_b[0], fresh_pair()
    for n in range(share):
        for u in range(2):
            product = dot(scaled, gates_b_all[n, u].reshape(slab, LANES))
            for g in range(SIDE):
                tile = product[g * TILE : (g + 1) * TILE]
                if u == 0:
                    tile = jnp.where(sub == GROUP, squares, tile)
                sz[n * SIDE + g, u] = tile.astype(BF16)
        send_pieces(ff_b, ff_sems, n * SIDE, (n + 1) * SIDE)
    lower = jnp.where(iota((slab, width), 0) == iota((slab, width), 1) + y * width, 1.0, 0.0).astype(BF16)
    residual = dot(mixed.astype(BF16), lower)
    hidden_units(ff_b, ff_sems, lambda piece: lax.rem(piece, SIDE))
    hidden = [
        ff_b[2][n * SIDE : (n + 1) * SIDE].astype(F32).reshape(ROWS, LANES).astype(BF16) for n in range(share)
    ]
    send_three, got_three = t_three
    for g in range(SIDE):
        partial = jnp.zeros((ROWS, width), F32)
        for n in range(share):
            partial = partial + dot_rows(hidden[n], down_b_all[n, g])
        send_three[g] = partial.reshape(SIDE, TILE, width).astype(BF16)
    got_three[y * tp_count + tp] = send_three[y]
    three_here = over_plane(lambda far: rows_of(send_three, far), got_three, rows_of)
    with jax.named_scope("plane_three"):
        three_here()
    summed = added(got_three, 0, SIDE * tp_count).reshape(ROWS, width)
    in_use = (iota((ROWS, width), 0) & 7) < GROUP
    last = jnp.where(in_use, residual + 0.5 * summed, 0.0).astype(BF16)

    back = iota((seqs, ROWS), 1)
    seat = lax.shift_right_logical(back, 3) * GROUP + (back & 7)
    lift = jnp.where(((back & 7) < GROUP) & (seat == iota((seqs, ROWS), 0)), 1.0, 0.0).astype(BF16)
    out_tile[...] = dot(lift, last).astype(BF16)
    out_copy = pltpu.make_async_copy(out_tile, out_ref, fresh_sem())
    out_copy.start()

    for condition, ref, sem in sent:
        if condition is None:
            take(ref, sem)
        else:

            @pl.when(condition)
            def _():
                take(ref, sem)

    out_copy.wait()


def on_device(
    ranks,
    tokens,
    gain_first,
    gate_first,
    up_first,
    down_first,
    gain_mixer,
    query_weight,
    key_weight,
    value_weight,
    forget_weight,
    forget_bias,
    key_cache,
    value_cache,
    forget_sum,
    out_weight,
    gain_second,
    gate_second,
    up_second,
    down_second,
):
    kv_count, tp_count = ranks
    depth = kv_count // SIDE
    seqs, length = key_cache.shape[:2]
    chunks = gate_first.shape[1] // LANES
    share = -(-chunks // SIDE)
    pieces = share * SIDE
    width = tokens.shape[1]
    slab = SIDE * width
    dma = pltpu.SemaphoreType.DMA

    def flat(cache):
        return cache.reshape(seqs, 2 * length, LANES)

    operands = [
        tokens,
        gain_first.reshape(1, -1),
        gate_first,
        up_first,
        down_first.T,
        gain_mixer.reshape(1, -1),
        query_weight,
        key_weight,
        value_weight,
        forget_weight.T,
        flat(key_cache),
        flat(value_cache),
        forget_sum,
        out_weight.T,
        gain_second.reshape(1, -1),
        gate_second,
        up_second,
        down_second.T,
    ]

    def half(*dims):
        return pltpu.VMEM(dims, BF16)

    def tiles(*dims):
        return pltpu.VMEM((*dims, TILE, LANES), BF16)

    def ff(count):
        return (tiles(count, 2), tiles(depth, 2), tiles(count))

    held = [
        pltpu.VMEM((1, forget_weight.shape[1]), F32),
        half(seqs, width),
        half(1, width),
        half(*gate_first.shape),
        half(*up_first.shape),
        half(1, width),
        half(1, width),
        half(forget_weight.shape[1], slab),
        half(seqs, 2 * length, LANES),
        half(seqs, 2 * length, LANES),
        pltpu.VMEM(forget_sum.shape, F32),
        half(pieces, 2, width, LANES),
        half(pieces, width, LANES),
        half(3, SIDE, width, 2 * LANES),
        half(SIDE, width, 2 * LANES),
        half(SIDE, width, chunks * LANES),
        half(share, 2, SIDE, width, LANES),
        half(share, SIDE, width, LANES),
        dma((17 + 2 * (-(-chunks // 4) + 23),)),
        (pltpu.SemaphoreType.REGULAR, pltpu.SemaphoreType.REGULAR),
        half(seqs, width),
        half(SIDE, TILE, width),
        half(SIDE, TILE, width),
        tiles(SIDE, chunks, 2),
        tiles(SIDE, chunks, 2),
        ff(chunks),
        ff(pieces),
        (
            tiles(depth, 2),
            tiles(depth, 4),
            tiles(SIDE, 2),
            tiles(SIDE, 2),
            tiles(SIDE, 2),
            pltpu.VMEM((SIDE, 1, LANES), F32),
            pltpu.VMEM((SIDE, 1, LANES), F32),
            tiles(depth, 2),
            pltpu.VMEM((depth, 1, LANES), F32),
        ),
        half(tp_count, TILE, slab),
        (half(TILE, slab), half(SIDE * tp_count, TILE, slab)),
        (half(SIDE, SIDE, TILE, width), half(SIDE * tp_count, SIDE, TILE, width)),
        half(SIDE, TILE, slab),
        pltpu.VMEM((SIDE, TILE, 2 * length), F32),
    ]
    return pl.pallas_call(
        functools.partial(layer_kernel, ranks, width * kv_count),
        out_shape=jax.ShapeDtypeStruct(tokens.shape, BF16),
        in_specs=[pl.BlockSpec(memory_space=pltpu.HBM)] * (1 + len(operands)),
        out_specs=pl.BlockSpec(memory_space=pltpu.HBM),
        scratch_shapes=held,
        compiler_params=pltpu.CompilerParams(
            collective_id=0, has_side_effects=True, vmem_limit_bytes=67_043_328
        ),
        name="layer",
    )(forget_bias.reshape(1, -1), *operands)


def solution(mesh):
    ranks = (mesh.shape["kv"], mesh.shape["tp"])
    kv, tp = "kv", "tp"
    in_specs = (
        P(None, kv),
        P(kv),
        P(kv, tp),
        P(kv, tp),
        P(tp, kv),
        P(kv),
        P(kv, tp),
        P(kv, tp),
        P(kv, tp),
        P(),
        P(),
        P(None, kv, tp, None),
        P(None, kv, tp, None),
        P(None, tp, kv),
        P(tp, kv),
        P(kv),
        P(kv, tp),
        P(kv, tp),
        P(tp, kv),
    )
    return jax.shard_map(
        functools.partial(on_device, ranks),
        mesh=mesh,
        in_specs=in_specs,
        out_specs=P(None, kv),
        check_vma=False,
    )
```
